32 devices in a mesh: kv: 16 (over z, y, x), tp: 2 (over core).
Axes of the slice: x: 2, y: 2, z: 4, core: 2. Of those that a mesh axis runs over, the one named last changes fastest.
Arguments:
- normed: bfloat16 [8192, 4096], P('kv'), may hold values from -6 to 6
- queries: bfloat16 [8192, 1024], P('kv', 'tp'), may hold values from -6 to 6
- keys: bfloat16 [8192, 64], P('kv'), may hold values from -6 to 6
- values: bfloat16 [8192, 64], P('kv'), may hold values from -6 to 6
- attended: bfloat16 [8192, 1024], P('kv', 'tp'), may hold values from -6 to 6
- cotangent: bfloat16 [8192, 1024], P('kv', 'tp'), may hold values from -24 to 24
- log_sum: float32 [8192, 16], P('kv', 'tp'), may hold values from 6 to 8
- chosen: int32 [128, 16], P('kv'), may hold values from -1 to 127, as said below
Outputs:
- grad_queries: bfloat16 [8192, 1024], P('kv', 'tp')
- grad_keys: float32 [8192, 64], P('kv')
- grad_values: float32 [8192, 64], P('kv')
- weight_grad: float32 [4096, 1024], P('kv', 'tp')
The draws below stay inside these ranges and needn't reach their ends.
Inputs may be any that keep to these rules, and one draw needn't show every extreme that they name: `chosen`: each row lists distinct key blocks, none after its own block, and always its own block; the listed entries come first and -1 fills the rest. A row lists from 8 to 16 blocks, fewer only where fewer blocks are open to it; on every index of kv some row lists 16 blocks where that many are open. The rows of one index of kv together list at most one block of each other index of kv's positions; every index of kv from 1 on lists a block of index 0 and a block of the index before it, and every index from half the axis on a block of the index half the axis before it.
All inputs are finite; a program needn't handle non-finite values.
Results may differ from the reference program's by a relative error of at most 0.007.
Values may be sent and summed in bfloat16 or wider, within the bound.
A program may use at most 64 MiB of HBM per device.

```python
import jax
import jax.numpy as jnp
from jax import lax

D = 4096
HEADS = 16
HEAD_DIM = 64
BLOCK = 64
NSEL = 16
LEAST = 8
TOK_DEV = 512
TOKENS = 8192


def draw_chosen(key, part):
    device_count = TOKENS // TOK_DEV
    per_device = TOK_DEV // BLOCK
    block_count = TOKENS // BLOCK
    first_key = jax.random.fold_in(key, 11)
    second_key = jax.random.fold_in(key, 12)
    third_key = jax.random.fold_in(key, 13)
    fourth_key = jax.random.fold_in(key, 14)
    offsets = jax.random.randint(first_key, (device_count, device_count), 0, per_device)
    row_ids = jnp.arange(block_count, dtype=jnp.int32)
    col_ids = jnp.arange(block_count, dtype=jnp.int32)
    row_dev = row_ids // per_device
    col_dev = col_ids // per_device
    fetched = col_dev[None, :] * per_device + offsets[row_dev[:, None], col_dev[None, :]]
    local_open = (col_dev[None, :] == row_dev[:, None]) & (col_ids[None, :] <= row_ids[:, None])
    remote_open = (col_dev[None, :] < row_dev[:, None]) & (col_ids[None, :] == fetched)
    is_open = local_open | remote_open
    near = (col_dev[None, :] == row_dev[:, None] - 1) | (col_dev[None, :] == row_dev[:, None] - device_count // 2) | (col_dev[None, :] == 0)
    forced = (col_ids[None, :] == row_ids[:, None]) | remote_open & near
    noise = jax.random.randint(second_key, (block_count, block_count), 0, 4096)
    ranked = jnp.where(forced, 2 ** 28 + col_ids[None, :], jnp.where(is_open, noise * block_count + col_ids[None, :], -1 - col_ids[None, :]))
    top_values, picked = lax.top_k(ranked, NSEL)
    span_size = NSEL - LEAST + 1
    first_draw = jax.random.randint(third_key, (block_count,), 0, span_size)
    second_draw = jax.random.randint(fourth_key, (block_count,), 0, span_size)
    listed_count = LEAST + jnp.minimum(first_draw, second_draw)
    listed_count = jnp.where(row_ids % per_device == per_device - 1, NSEL, listed_count)
    slot_ids = jnp.arange(NSEL, dtype=jnp.int32)
    keep = (slot_ids[None, :] < listed_count[:, None]) & (top_values >= 0)
    return jnp.where(keep, picked, -1).astype(jnp.int32)


def strengthened(entries, stream_key, source, target, blocks, factor):
    def block_of(dim):
        return (jnp.arange(entries.shape[dim]) // (entries.shape[dim] // blocks)).reshape((-1,) + (1,) * (entries.ndim - 1 - dim))

    first = jax.random.permutation(stream_key, blocks)[block_of(target)]
    other_side = (block_of(target) + blocks // 2) % blocks
    return jnp.where((block_of(source) == first) | (block_of(source) == other_side), factor * entries, entries)


def block_levels(key, shape, pieces, smallest, largest):
    level = 1.0
    for position, blocks in pieces:
        heights = jax.random.uniform(jax.random.fold_in(jax.random.fold_in(key, 6), position), (blocks,), jnp.float32, smallest / len(pieces), largest / len(pieces))
        level = level * jnp.repeat(jnp.exp(heights), shape[position] // blocks).reshape((-1,) + (1,) * (len(shape) - 1 - position))
    return level


def scatter_about(stream_key, extent, scale, reach, shards=(), kind=jnp.bfloat16):
    entries = jax.random.normal(stream_key, extent, jnp.float32) * scale
    if len(shards) > 0:
        entries = block_levels(stream_key, extent, shards, -0.22, 0.18) * entries
    return jnp.clip(entries, min=-reach, max=reach).astype(kind)


def noise_with(stream_key, shape, deviation, reach, cuts, heavy, held_as=jnp.bfloat16):
    values = deviation * jax.random.normal(stream_key, shape, jnp.float32)
    if cuts:
        values = values * block_levels(stream_key, shape, cuts, -0.22, 0.18)
    return jnp.clip(strengthened(values, jax.random.fold_in(stream_key, 3), *heavy), -reach, reach).astype(held_as)


def setup_inputs(seed: int = 0) -> dict:
    key_list = jax.random.split(jax.random.key(seed), 9)
    normed = noise_with(key_list[0], (TOKENS, D), 1.0, 6.0, ((0, 16),), (0, 1, 16, 2.0))
    queries = scatter_about(key_list[1], (TOKENS, HEADS * HEAD_DIM), 1.0, 6.0, ((0, 16), (1, 2)))
    keys = scatter_about(key_list[2], (TOKENS, HEAD_DIM), 1.0, 6.0, ((0, 16),))
    values = scatter_about(key_list[3], (TOKENS, HEAD_DIM), 1.0, 6.0, ((0, 16),))
    attended = scatter_about(key_list[4], (TOKENS, HEADS * HEAD_DIM), 1.0, 6.0, ((0, 16), (1, 2)))
    cotangent = scatter_about(key_list[5], (TOKENS, HEADS * HEAD_DIM), 4.0, 24.0, ((0, 16), (1, 2)))
    log_sum = jnp.clip(6.0 + 2.0 * jax.random.uniform(key_list[6], (TOKENS, HEADS), jnp.float32) ** block_levels(key_list[6], (TOKENS, HEADS), ((0, 16), (1, 2)), -0.2, 0.2), 6.0, 8.0)
    chosen = draw_chosen(jax.random.fold_in(key_list[8], 71), 0)
    return {"normed": normed, "queries": queries, "keys": keys, "values": values, "attended": attended, "cotangent": cotangent, "log_sum": log_sum, "chosen": chosen}


def reference(normed, queries, keys, values, attended, cotangent, log_sum, chosen):
    block_count = TOKENS // BLOCK
    score_scale = HEAD_DIM ** -0.5
    query_matrix = queries.reshape(block_count, BLOCK, HEADS, HEAD_DIM)
    gradient_rows = cotangent.reshape(block_count, BLOCK, HEADS, HEAD_DIM)
    out_rows = attended.reshape(block_count, BLOCK, HEADS, HEAD_DIM)
    log_rows = log_sum.reshape(block_count, BLOCK, HEADS)
    pair_rows = jnp.concatenate([keys, values], axis=1).reshape(block_count, BLOCK, 2 * HEAD_DIM)
    offsets = jnp.arange(BLOCK, dtype=jnp.int32)

    def one_block(accumulated, block_id):
        listed_ids = chosen[block_id]
        listed = listed_ids >= 0
        safe_ids = jnp.where(listed, listed_ids, 0).astype(jnp.int32)
        picked = pair_rows[safe_ids].reshape(NSEL * BLOCK, 2 * HEAD_DIM).astype(jnp.float32)
        selected_keys = picked[:, :HEAD_DIM]
        selected_values = picked[:, HEAD_DIM:]
        query_block = query_matrix[block_id].astype(jnp.float32)
        grad_block = gradient_rows[block_id].astype(jnp.float32)
        out_block = out_rows[block_id].astype(jnp.float32)
        key_pos = (safe_ids[:, None] * BLOCK + offsets[None, :]).reshape(NSEL * BLOCK)
        key_live = jnp.repeat(listed, BLOCK)
        query_pos = block_id * BLOCK + offsets
        allowed = key_live[None, :] & (key_pos[None, :] <= query_pos[:, None])
        scores = jnp.einsum('thd,kd->htk', query_block, selected_keys) * score_scale
        probs = jnp.where(allowed[None], jnp.exp(scores - log_rows[block_id].T[:, :, None]), 0.0)
        reduced_probabilities = lax.optimization_barrier(probs.astype(jnp.bfloat16)).astype(jnp.float32)
        grad_value = jnp.einsum('htk,thd->kd', reduced_probabilities, grad_block)
        probability_gradient = jnp.einsum('thd,kd->htk', grad_block, selected_values)
        deltas = jnp.sum(grad_block * out_block, axis=-1).T
        score_gradient = (probs * (probability_gradient - deltas[:, :, None]) * score_scale).astype(jnp.bfloat16)
        dscores_wide = lax.optimization_barrier(score_gradient).astype(jnp.float32)
        query_gradient = jnp.einsum('htk,kd->thd', dscores_wide, selected_keys).astype(jnp.bfloat16)
        key_gradient = jnp.einsum('htk,thd->kd', dscores_wide, query_block)
        terms = jnp.concatenate([key_gradient, grad_value], axis=1).reshape(NSEL, BLOCK, 2 * HEAD_DIM)
        terms = jnp.where(listed[:, None, None], terms, 0.0)
        accumulated = accumulated.at[safe_ids].add(terms)
        return accumulated, query_gradient.reshape(BLOCK, HEADS * HEAD_DIM)

    initial = jnp.zeros((block_count, BLOCK, 2 * HEAD_DIM), jnp.float32)
    accumulated, grad_blocks = lax.scan(one_block, initial, jnp.arange(block_count, dtype=jnp.int32))
    grad_queries = grad_blocks.reshape(TOKENS, HEADS * HEAD_DIM)
    grad_keys = accumulated[:, :, :HEAD_DIM].reshape(TOKENS, HEAD_DIM)
    grad_values = accumulated[:, :, HEAD_DIM:].reshape(TOKENS, HEAD_DIM)
    weight_grad = jnp.dot(normed.T, grad_queries, preferred_element_type=jnp.float32)
    return grad_queries, grad_keys, grad_values, weight_grad
```

```python
import functools

import jax
import jax.numpy as jnp
from jax import lax
from jax.experimental import pallas as pl
from jax.experimental.pallas import tpu as pltpu
from jax.sharding import PartitionSpec as P

BLOCK = 64
GROUP = 4
NT = (((1,), (1,)), ((), ()))
TN = (((0,), (0,)), ((), ()))


def greet(n, peers_tp):
    me = lax.axis_index("kv")
    barrier = pltpu.get_barrier_semaphore()

    def hello(k, _):
        pl.semaphore_signal(barrier, inc=1, device_id={"kv": lax.rem(me + k, n)})
        return 0

    lax.fori_loop(1, n, hello, 0)
    if peers_tp > 1:
        mine = lax.axis_index("tp")
        for k in range(1, peers_tp):
            pl.semaphore_signal(
                barrier, inc=1, device_id={"tp": lax.rem(mine + k, peers_tp)}
            )
    return barrier


def fetch_kernel(n, nb, keys_ref, values_ref, want_ref, table_ref, asked_ref, out_buf, s1, r1, s2, r2):
    me = lax.axis_index("kv")
    barrier = greet(n, 1)
    pairs = jnp.concatenate([keys_ref[...], values_ref[...]], axis=1)
    for b in range(nb):
        table_ref[b] = pairs[b * BLOCK : (b + 1) * BLOCK]

    def blank(p, _):
        table_ref[nb + p] = jnp.zeros(table_ref.shape[1:], table_ref.dtype)
        return 0

    lax.fori_loop(me, n, blank, 0)

    def unasked(p, _):
        asked_ref[p] = jnp.full(asked_ref.shape[1:], -1, jnp.int32)
        return 0

    lax.fori_loop(0, me + 1, unasked, 0)
    pl.semaphore_wait(barrier, n - 1)

    def request(p):
        return pltpu.make_async_remote_copy(
            src_ref=want_ref.at[p],
            dst_ref=asked_ref.at[me],
            send_sem=s1.at[p],
            recv_sem=r1.at[me],
            device_id={"kv": p},
        )

    def asked_from(q):
        return pltpu.make_async_remote_copy(
            src_ref=want_ref.at[q],
            dst_ref=asked_ref.at[q],
            send_sem=s1.at[q],
            recv_sem=r1.at[q],
            device_id={"kv": q},
        )

    def reply(q):
        return pltpu.make_async_remote_copy(
            src_ref=out_buf.at[q],
            dst_ref=table_ref.at[nb + me],
            send_sem=s2.at[q],
            recv_sem=r2.at[me],
            device_id={"kv": q},
        )

    def reply_from(p):
        return pltpu.make_async_remote_copy(
            src_ref=out_buf.at[p],
            dst_ref=table_ref.at[nb + p],
            send_sem=s2.at[p],
            recv_sem=r2.at[p],
            device_id={"kv": p},
        )

    def step(fn):
        def body(i, _):
            fn(i)
            return 0

        return body

    lax.fori_loop(0, me, step(lambda p: request(p).start()), 0)

    def answer(q):
        asked_from(q).wait_recv()
        tile = asked_ref[q]
        wide = jnp.concatenate([tile] * (BLOCK // tile.shape[0]), axis=0)
        picked = jnp.zeros(wide.shape, jnp.float32)
        for b in range(nb):
            picked = jnp.where(wide == b, table_ref[b].astype(jnp.float32), picked)
        out_buf[q] = picked.astype(out_buf.dtype)
        reply(q).start()

    lax.fori_loop(me + 1, n, step(answer), 0)
    lax.fori_loop(0, me, step(lambda p: request(p).wait_send()), 0)
    lax.fori_loop(me + 1, n, step(lambda q: reply(q).wait_send()), 0)
    lax.fori_loop(0, me, step(lambda p: reply_from(p).wait_recv()), 0)


def attention_kernel(
    heads, nb, n, slots, limits, counts,
    q_ref, o_ref, g_ref, l_ref, table_ref, gq_ref, own_ref, back_ref, acc, dqt,
):
    g = pl.program_id(0)
    rows = heads * BLOCK
    scale = BLOCK ** (-0.5)

    @pl.when(g == 0)
    def _():
        acc[...] = jnp.zeros_like(acc)

    def stack(ref):
        full = ref[...]
        return jnp.concatenate([full[:, h * BLOCK : (h + 1) * BLOCK] for h in range(heads)], axis=0)

    q = stack(q_ref)
    go = stack(g_ref)
    prod = go.astype(jnp.float32) * stack(o_ref).astype(jnp.float32)
    high = prod.astype(jnp.bfloat16)
    low = (prod - high.astype(jnp.float32)).astype(jnp.bfloat16)
    ones = jnp.ones((8, BLOCK), jnp.bfloat16)
    delta = (
        lax.dot_general(ones, high, NT, preferred_element_type=jnp.float32)
        + lax.dot_general(ones, low, NT, preferred_element_type=jnp.float32)
    )[0:1]
    logs = l_ref[0]
    ahead = (
        lax.broadcasted_iota(jnp.int32, (BLOCK, rows), 1) % BLOCK
        - lax.broadcasted_iota(jnp.int32, (BLOCK, rows), 0)
    )
    dqt[...] = jnp.zeros_like(dqt)
    for c in range(slots.shape[1] // GROUP):

        @pl.when(counts[g] > c * GROUP)
        def _():
            ids = [slots[g, c * GROUP + i] for i in range(GROUP)]
            pairs = jnp.concatenate([table_ref[s] for s in ids], axis=0)
            k = pairs[:, :BLOCK]
            v = pairs[:, BLOCK:]
            s = lax.dot_general(k, q, NT, preferred_element_type=jnp.float32)
            dp = lax.dot_general(v, go, NT, preferred_element_type=jnp.float32)
            e = jnp.exp(s * scale - logs)
            p = jnp.concatenate(
                [
                    jnp.where(
                        ahead >= limits[g, c * GROUP + i], e[i * BLOCK : (i + 1) * BLOCK], 0.0
                    )
                    for i in range(GROUP)
                ],
                axis=0,
            )
            ds = (p * (dp - delta) * scale).astype(jnp.bfloat16)
            dk = jnp.dot(ds, q, preferred_element_type=jnp.float32)
            dv = jnp.dot(p.astype(jnp.bfloat16), go, preferred_element_type=jnp.float32)
            dqt[...] += lax.dot_general(k, ds, TN, preferred_element_type=jnp.float32)
            dkv = jnp.concatenate([dk, dv], axis=1)
            for i in range(GROUP):
                acc[ids[i]] += dkv[i * BLOCK : (i + 1) * BLOCK]

    dq = dqt[...].T.astype(jnp.bfloat16)
    gq_ref[...] = jnp.concatenate([dq[h * BLOCK : (h + 1) * BLOCK] for h in range(heads)], axis=1)

    @pl.when(g == nb - 1)
    def _():
        own_ref[...] = acc[:nb]
        back_ref[...] = acc[nb:].astype(back_ref.dtype)


def reduce_kernel(
    n, tp, nb, normed_ref, gq_ref, own_ref, back_ref, asked_ref,
    wg_ref, dk_ref, dv_ref,
    gqt, send1, recv1, own, send2, recv2, send3, recv3, came, total, others,
    ss1, rs1, ss2, rs2, ss3, rs3, ssb, rsb, sst, rst,
):
    me = lax.axis_index("kv")
    mine = lax.axis_index("tp")
    zs = n // 4
    x = lax.rem(me, 2)
    y = lax.rem(me // 2, 2)
    z = me // 4
    barrier = greet(n, tp)
    half = gqt.shape[1]
    width = send1.shape[3]
    turned = gq_ref[...].T
    gqt[0] = turned[:half]
    gqt[1] = turned[half:]

    def index(zz, a, b, h):
        return zz * 4 + (b * 2 + a if h == 0 else a * 2 + b)

    coords = ((x, y), (y, x))

    def chunk_at(h, i, a):
        b = coords[h][1]
        bb = jnp.where(i < zs, 1 - b, b)
        zz = lax.rem(z + 1 + lax.rem(i, zs), zs)
        return index(zz, a, bb, h)

    def part(h, chunk):
        cols = pl.ds(pl.multiple_of(chunk * width, 128), width)
        return jnp.dot(gqt[h], normed_ref[:, cols], preferred_element_type=jnp.float32)

    def copy1(h, i):
        a, b = coords[h]
        return pltpu.make_async_remote_copy(
            src_ref=send1.at[h, i], dst_ref=recv1.at[h, i],
            send_sem=ss1.at[h, i], recv_sem=rs1.at[h, i],
            device_id={"kv": index(z, 1 - a, b, h)},
        )

    def copy2(h, i):
        a, b = coords[h]
        return pltpu.make_async_remote_copy(
            src_ref=send2.at[h, i], dst_ref=recv2.at[h, i],
            send_sem=ss2.at[h, i], recv_sem=rs2.at[h, i],
            device_id={"kv": index(z, a, 1 - b, h)},
        )

    def copy3(h, i):
        a, b = coords[h]
        return pltpu.make_async_remote_copy(
            src_ref=send3.at[h, i], dst_ref=recv3.at[h, i],
            send_sem=ss3.at[h, i], recv_sem=rs3.at[h, i],
            device_id={"kv": index(lax.rem(z + 1 + i, zs), a, b, h)},
        )

    def back_to(p):
        return pltpu.make_async_remote_copy(
            src_ref=back_ref.at[p], dst_ref=came.at[me],
            send_sem=ssb.at[p], recv_sem=rsb.at[me], device_id={"kv": p},
        )

    def back_from(q):
        return pltpu.make_async_remote_copy(
            src_ref=back_ref.at[q], dst_ref=came.at[q],
            send_sem=ssb.at[q], recv_sem=rsb.at[q], device_id={"kv": q},
        )

    def across(k):
        return pltpu.make_async_remote_copy(
            src_ref=total, dst_ref=others.at[k - 1],
            send_sem=sst.at[k - 1], recv_sem=rst.at[k - 1],
            device_id={"tp": lax.rem(mine + k, tp)},
        )

    def loop(start, stop, fn):
        def body(i, _):
            fn(i)
            return 0

        lax.fori_loop(start, stop, body, 0)

    def prepare(i):
        for h in range(2):
            send1[h, i] = part(h, chunk_at(h, i, 1 - coords[h][0])).astype(send1.dtype)

    prepare(0)
    pl.semaphore_wait(barrier, n - 1 + tp - 1)
    for h in range(2):
        copy1(h, 0).start()

    def first(i):
        prepare(i)
        for h in range(2):
            copy1(h, i).start()

    loop(1, 2 * zs, first)
    loop(0, me, lambda p: back_to(p).start())

    def keep(i):
        for h in range(2):
            own[h, i] = part(h, chunk_at(h, i, coords[h][0]))

    loop(0, 2 * zs, keep)

    def second(i):
        for h in range(2):
            copy1(h, i).wait_recv()
            send2[h, i] = (own[h, i] + recv1[h, i].astype(jnp.float32)).astype(send2.dtype)
            copy2(h, i).start()

    loop(0, zs, second)

    total[...] = own_ref[...]

    def gather(q):
        back_from(q).wait_recv()
        tile = asked_ref[q]
        wide = jnp.concatenate([tile] * (BLOCK // tile.shape[0]), axis=0)
        block = came[q].astype(jnp.float32)
        for b in range(nb):
            total[b] += jnp.where(wide == b, block, 0.0)

    loop(me + 1, n, gather)
    for k in range(1, tp):
        across(k).start()

    def joined(h, i):
        copy1(h, zs + i).wait_recv()
        copy2(h, i).wait_recv()
        return (
            own[h, zs + i]
            + recv1[h, zs + i].astype(jnp.float32)
            + recv2[h, i].astype(jnp.float32)
        )

    def third(i):
        for h in range(2):
            send3[h, i] = joined(h, i).astype(send3.dtype)
            copy3(h, i).start()

    loop(0, zs - 1, third)

    for k in range(1, tp):
        across(k).wait_recv()
    summed = total[...]
    for k in range(1, tp):
        summed = summed + others[k - 1]
    flat = summed.reshape(nb * BLOCK, 2 * BLOCK)
    dk_ref[...] = flat[:, :BLOCK]
    dv_ref[...] = flat[:, BLOCK:]

    for h in range(2):
        own[h, 0] = joined(h, zs - 1)

    def fourth(i):
        for h in range(2):
            copy3(h, i).wait_recv()
            own[h, 0] += recv3[h, i].astype(jnp.float32)

    loop(0, zs - 1, fourth)
    whole = jnp.concatenate([own[0, 0], own[1, 0]], axis=0)
    wg_ref[...] = whole.T

    for h in range(2):
        loop(0, 2 * zs, lambda i: copy1(h, i).wait_send())
        loop(0, zs, lambda i: copy2(h, i).wait_send())
        loop(0, zs - 1, lambda i: copy3(h, i).wait_send())
    loop(0, me, lambda p: back_to(p).wait_send())
    for k in range(1, tp):
        across(k).wait_send()


def shards(n, tp, normed, queries, keys, values, attended, cotangent, log_sum, chosen):
    me = lax.axis_index("kv")
    tok_rows, model_width = normed.shape
    slot_count = chosen.shape[1]
    nb = tok_rows // BLOCK
    heads = log_sum.shape[1]
    cols = queries.shape[1]
    pair = 2 * BLOCK
    vmem = pl.BlockSpec(memory_space=pltpu.VMEM)
    dma = pltpu.SemaphoreType.DMA

    owners = chosen // nb
    within = chosen % nb
    listed = chosen >= 0
    remote = listed & (owners != me)
    peer_ids = jnp.arange(n, dtype=jnp.int32)
    matched = remote[:, :, None] & (owners[:, :, None] == peer_ids)
    wanted = jnp.max(jnp.where(matched, within[:, :, None], -1), axis=(0, 1))
    wanted = jnp.broadcast_to(wanted[:, None, None], (n, 8, 128))
    slots = jnp.where(listed, jnp.where(owners == me, within, nb + owners), 0)
    row_base = (me * nb + jnp.arange(nb, dtype=jnp.int32))[:, None]
    limits = jnp.where(listed, (chosen - row_base) * BLOCK, 4 * BLOCK)
    counts = jnp.sum(listed.astype(jnp.int32), axis=1)

    table, asked = pl.pallas_call(
        functools.partial(fetch_kernel, n, nb),
        out_shape=(
            jax.ShapeDtypeStruct((nb + n, BLOCK, pair), jnp.bfloat16),
            jax.ShapeDtypeStruct((n, 8, 128), jnp.int32),
        ),
        in_specs=[vmem] * 3,
        out_specs=(vmem, vmem),
        scratch_shapes=[pltpu.VMEM((n, BLOCK, pair), jnp.bfloat16)] + [dma((n,))] * 4,
        compiler_params=pltpu.CompilerParams(collective_id=0, has_side_effects=True),
        name="fetch",
    )(keys, values, wanted)

    logs = log_sum.reshape(nb, BLOCK, heads).transpose(0, 2, 1).reshape(nb, 1, heads * BLOCK)
    rows_spec = pl.BlockSpec((BLOCK, cols), lambda g, *_: (g, 0))
    gq, own_part, back = pl.pallas_call(
        functools.partial(attention_kernel, heads, nb, n),
        out_shape=(
            jax.ShapeDtypeStruct((tok_rows, cols), jnp.bfloat16),
            jax.ShapeDtypeStruct((nb, BLOCK, pair), jnp.float32),
            jax.ShapeDtypeStruct((n, BLOCK, pair), jnp.bfloat16),
        ),
        grid_spec=pltpu.PrefetchScalarGridSpec(
            num_scalar_prefetch=3,
            grid=(nb,),
            in_specs=[
                rows_spec,
                rows_spec,
                rows_spec,
                pl.BlockSpec((1, 1, heads * BLOCK), lambda g, *_: (g, 0, 0)),
                pl.BlockSpec((nb + n, BLOCK, pair), lambda g, *_: (0, 0, 0)),
            ],
            out_specs=(
                rows_spec,
                pl.BlockSpec((nb, BLOCK, pair), lambda g, *_: (0, 0, 0)),
                pl.BlockSpec((n, BLOCK, pair), lambda g, *_: (0, 0, 0)),
            ),
            scratch_shapes=[
                pltpu.VMEM((nb + n, BLOCK, pair), jnp.float32),
                pltpu.VMEM((BLOCK, heads * BLOCK), jnp.float32),
            ],
        ),
        compiler_params=pltpu.CompilerParams(dimension_semantics=("arbitrary",)),
        name="attention",
    )(slots, limits, counts, queries, attended, cotangent, logs, table)

    zs = n // 4
    half = cols // 2
    width = model_width // n
    low = jnp.bfloat16
    wide = jnp.float32
    weight_grad, grad_keys, grad_values = pl.pallas_call(
        functools.partial(reduce_kernel, n, tp, nb),
        out_shape=(
            jax.ShapeDtypeStruct((width, cols), wide),
            jax.ShapeDtypeStruct((tok_rows, BLOCK), wide),
            jax.ShapeDtypeStruct((tok_rows, BLOCK), wide),
        ),
        in_specs=[vmem] * 5,
        out_specs=(vmem, vmem, vmem),
        scratch_shapes=[
            pltpu.VMEM((2, half, tok_rows), low),
            pltpu.VMEM((2, 2 * zs, half, width), low),
            pltpu.VMEM((2, 2 * zs, half, width), low),
            pltpu.VMEM((2, 2 * zs, half, width), wide),
            pltpu.VMEM((2, zs, half, width), low),
            pltpu.VMEM((2, zs, half, width), low),
            pltpu.VMEM((2, zs - 1, half, width), low),
            pltpu.VMEM((2, zs - 1, half, width), low),
            pltpu.VMEM((n, BLOCK, pair), low),
            pltpu.VMEM((nb, BLOCK, pair), wide),
            pltpu.VMEM((tp - 1, nb, BLOCK, pair), wide),
            dma((2, 2 * zs)), dma((2, 2 * zs)),
            dma((2, zs)), dma((2, zs)),
            dma((2, zs - 1)), dma((2, zs - 1)),
            dma((n,)), dma((n,)),
            dma((tp - 1,)), dma((tp - 1,)),
        ],
        compiler_params=pltpu.CompilerParams(
            collective_id=1, has_side_effects=True, vmem_limit_bytes=56 * 1024 * 1024
        ),
        name="reduce",
    )(normed, gq, own_part, back, asked)
    return (gq, grad_keys, grad_values, weight_grad)


def solution(mesh):
    placed = (
        P("kv", None),
        P("kv", "tp"),
        P("kv", None),
        P("kv", None),
        P("kv", "tp"),
        P("kv", "tp"),
        P("kv", "tp"),
        P("kv", None),
    )
    return jax.shard_map(
        functools.partial(shards, mesh.shape["kv"], mesh.shape["tp"]),
        mesh=mesh,
        in_specs=placed,
        out_specs=(P("kv", "tp"), P("kv", None), P("kv", None), P("kv", "tp")),
        check_vma=False,
    )
```

```python
import functools

import jax
import jax.numpy as jnp
from jax import lax
from jax.experimental import pallas as pl
from jax.experimental.pallas import tpu as pltpu
from jax.sharding import PartitionSpec as P

BLOCK = 64
GROUP = 4
ROUNDS = 2
NT = (((1,), (1,)), ((), ()))
TN = (((0,), (0,)), ((), ()))


def greet(n, peers_tp):
    me = lax.axis_index("kv")
    barrier = pltpu.get_barrier_semaphore()

    def hello(k, _):
        pl.semaphore_signal(barrier, inc=1, device_id={"kv": lax.rem(me + k, n)})
        return 0

    lax.fori_loop(1, n, hello, 0)
    if peers_tp > 1:
        mine = lax.axis_index("tp")
        for k in range(1, peers_tp):
            pl.semaphore_signal(
                barrier, inc=1, device_id={"tp": lax.rem(mine + k, peers_tp)}
            )
    return barrier


def fetch_kernel(n, nb, keys_ref, values_ref, want_ref, table_ref, asked_ref, out_buf, s1, r1, s2, r2):
    me = lax.axis_index("kv")
    barrier = greet(n, 1)
    pairs = jnp.concatenate([keys_ref[...], values_ref[...]], axis=0).T
    for b in range(nb):
        table_ref[b] = pairs[b * BLOCK : (b + 1) * BLOCK]

    def blank(p, _):
        table_ref[nb + p] = jnp.zeros(table_ref.shape[1:], table_ref.dtype)
        return 0

    lax.fori_loop(me, n, blank, 0)

    def unasked(p, _):
        asked_ref[p] = jnp.full(asked_ref.shape[1:], -1, jnp.int32)
        return 0

    lax.fori_loop(0, me + 1, unasked, 0)
    pl.semaphore_wait(barrier, n - 1)

    def request(p):
        return pltpu.make_async_remote_copy(
            src_ref=want_ref.at[p],
            dst_ref=asked_ref.at[me],
            send_sem=s1.at[p],
            recv_sem=r1.at[me],
            device_id={"kv": p},
        )

    def asked_from(q):
        return pltpu.make_async_remote_copy(
            src_ref=want_ref.at[q],
            dst_ref=asked_ref.at[q],
            send_sem=s1.at[q],
            recv_sem=r1.at[q],
            device_id={"kv": q},
        )

    def reply(q):
        return pltpu.make_async_remote_copy(
            src_ref=out_buf.at[q],
            dst_ref=table_ref.at[nb + me],
            send_sem=s2.at[q],
            recv_sem=r2.at[me],
            device_id={"kv": q},
        )

    def reply_from(p):
        return pltpu.make_async_remote_copy(
            src_ref=out_buf.at[p],
            dst_ref=table_ref.at[nb + p],
            send_sem=s2.at[p],
            recv_sem=r2.at[p],
            device_id={"kv": p},
        )

    def step(fn):
        def body(i, _):
            fn(i)
            return 0

        return body

    lax.fori_loop(0, me, step(lambda p: request(p).start()), 0)

    def answer(q):
        asked_from(q).wait_recv()
        tile = asked_ref[q]
        wide = jnp.concatenate([tile] * (BLOCK // tile.shape[0]), axis=0)
        picked = jnp.zeros(wide.shape, jnp.float32)
        for b in range(nb):
            picked = jnp.where(wide == b, table_ref[b].astype(jnp.float32), picked)
        out_buf[q] = picked.astype(out_buf.dtype)
        reply(q).start()

    lax.fori_loop(me + 1, n, step(answer), 0)
    lax.fori_loop(0, me, step(lambda p: request(p).wait_send()), 0)
    lax.fori_loop(me + 1, n, step(lambda q: reply(q).wait_send()), 0)
    lax.fori_loop(0, me, step(lambda p: reply_from(p).wait_recv()), 0)


def attention_kernel(
    heads, nb, n, slots, limits, counts,
    q_ref, o_ref, g_ref, l_ref, table_ref, gq_ref, own_ref, back_ref, acc, dqt,
):
    g = pl.program_id(0)
    rows = heads * BLOCK
    scale = BLOCK ** (-0.5)

    @pl.when(g == 0)
    def _():
        acc[...] = jnp.zeros_like(acc)

    def stack(ref):
        full = ref[...]
        return jnp.concatenate([full[:, h * BLOCK : (h + 1) * BLOCK] for h in range(heads)], axis=0)

    q = stack(q_ref)
    go = stack(g_ref)
    prod = go.astype(jnp.float32) * stack(o_ref).astype(jnp.float32)
    high = prod.astype(jnp.bfloat16)
    low = (prod - high.astype(jnp.float32)).astype(jnp.bfloat16)
    ones = jnp.ones((8, BLOCK), jnp.bfloat16)
    delta = (
        lax.dot_general(ones, high, NT, preferred_element_type=jnp.float32)
        + lax.dot_general(ones, low, NT, preferred_element_type=jnp.float32)
    )[0:1]
    logs = l_ref[0]
    ahead = (
        lax.broadcasted_iota(jnp.int32, (BLOCK, rows), 1) % BLOCK
        - lax.broadcasted_iota(jnp.int32, (BLOCK, rows), 0)
    )
    dqt[...] = jnp.zeros_like(dqt)
    for c in range(slots.shape[1] // GROUP):

        @pl.when(counts[g] > c * GROUP)
        def _():
            ids = [slots[g, c * GROUP + i] for i in range(GROUP)]
            pairs = jnp.concatenate([table_ref[s] for s in ids], axis=0)
            k = pairs[:, :BLOCK]
            v = pairs[:, BLOCK:]
            s = lax.dot_general(k, q, NT, preferred_element_type=jnp.float32)
            dp = lax.dot_general(v, go, NT, preferred_element_type=jnp.float32)
            e = jnp.exp(s * scale - logs)
            p = jnp.concatenate(
                [
                    jnp.where(
                        ahead >= limits[g, c * GROUP + i], e[i * BLOCK : (i + 1) * BLOCK], 0.0
                    )
                    for i in range(GROUP)
                ],
                axis=0,
            )
            ds = (p * (dp - delta) * scale).astype(jnp.bfloat16)
            dk = jnp.dot(ds, q, preferred_element_type=jnp.float32)
            dv = jnp.dot(p.astype(jnp.bfloat16), go, preferred_element_type=jnp.float32)
            dqt[...] += lax.dot_general(k, ds, TN, preferred_element_type=jnp.float32)
            dkv = jnp.concatenate([dk, dv], axis=1)
            for i in range(GROUP):
                acc[ids[i]] += dkv[i * BLOCK : (i + 1) * BLOCK]

    dq = dqt[...].T.astype(jnp.bfloat16)
    gq_ref[...] = jnp.concatenate([dq[h * BLOCK : (h + 1) * BLOCK] for h in range(heads)], axis=1)

    @pl.when(g == nb - 1)
    def _():
        own_ref[...] = acc[:nb]
        back_ref[...] = acc[nb:].astype(back_ref.dtype)


def reduce_kernel(
    n, tp, nb, rounds, normed_ref, gq_ref, own_ref, back_ref, asked_ref,
    wg_ref, dk_ref, dv_ref,
    gqt, send1, recv1, own, send2, recv2, send3, recv3, came, total, others,
    ss1, rs1, ss2, rs2, ss3, rs3, ssb, rsb, sst, rst,
):
    me = lax.axis_index("kv")
    mine = lax.axis_index("tp")
    zs = n // 4
    x = lax.rem(me, 2)
    y = lax.rem(me // 2, 2)
    z = me // 4
    barrier = greet(n, tp)
    rows = gqt.shape[2]
    width = send1.shape[4]
    turned = gq_ref[...].T
    for r in range(rounds):
        for h in range(2):
            gqt[h, r] = turned[(2 * r + h) * rows : (2 * r + h + 1) * rows]

    def index(zz, a, b, h):
        return zz * 4 + (b * 2 + a if h == 0 else a * 2 + b)

    coords = ((x, y), (y, x))

    def chunk_at(h, i, a):
        b = coords[h][1]
        bb = jnp.where(i < zs, 1 - b, b)
        zz = lax.rem(z + 1 + lax.rem(i, zs), zs)
        return index(zz, a, bb, h)

    def part(h, r, chunk):
        cols = pl.ds(pl.multiple_of(chunk * width, 128), width)
        return jnp.dot(gqt[h, r], normed_ref[:, cols], preferred_element_type=jnp.float32)

    def copy1(h, r, i):
        a, b = coords[h]
        return pltpu.make_async_remote_copy(
            src_ref=send1.at[h, r, i], dst_ref=recv1.at[h, r, i],
            send_sem=ss1.at[h, r, i], recv_sem=rs1.at[h, r, i],
            device_id={"kv": index(z, 1 - a, b, h)},
        )

    def copy2(h, r, i):
        a, b = coords[h]
        return pltpu.make_async_remote_copy(
            src_ref=send2.at[h, r, i], dst_ref=recv2.at[h, r, i],
            send_sem=ss2.at[h, r, i], recv_sem=rs2.at[h, r, i],
            device_id={"kv": index(z, a, 1 - b, h)},
        )

    def copy3(h, r, i):
        a, b = coords[h]
        return pltpu.make_async_remote_copy(
            src_ref=send3.at[h, r, i], dst_ref=recv3.at[h, r, i],
            send_sem=ss3.at[h, r, i], recv_sem=rs3.at[h, r, i],
            device_id={"kv": index(lax.rem(z + 1 + i, zs), a, b, h)},
        )

    def back_to(p):
        return pltpu.make_async_remote_copy(
            src_ref=back_ref.at[p], dst_ref=came.at[me],
            send_sem=ssb.at[p], recv_sem=rsb.at[me], device_id={"kv": p},
        )

    def back_from(q):
        return pltpu.make_async_remote_copy(
            src_ref=back_ref.at[q], dst_ref=came.at[q],
            send_sem=ssb.at[q], recv_sem=rsb.at[q], device_id={"kv": q},
        )

    def across(k):
        return pltpu.make_async_remote_copy(
            src_ref=total, dst_ref=others.at[k - 1],
            send_sem=sst.at[k - 1], recv_sem=rst.at[k - 1],
            device_id={"tp": lax.rem(mine + k, tp)},
        )

    def loop(start, stop, fn):
        def body(i, _):
            fn(i)
            return 0

        lax.fori_loop(start, stop, body, 0)

    def prepare(r, i):
        for h in range(2):
            send1[h, r, i] = part(h, r, chunk_at(h, i, 1 - coords[h][0])).astype(send1.dtype)

    def first(r, i):
        prepare(r, i)
        for h in range(2):
            copy1(h, r, i).start()

    def second(r, i):
        for h in range(2):
            mine_here = part(h, r, chunk_at(h, i, coords[h][0]))
            copy1(h, r, i).wait_recv()
            send2[h, r, i] = (mine_here + recv1[h, r, i].astype(jnp.float32)).astype(send2.dtype)
            copy2(h, r, i).start()
        first(r, zs + i)
        for h in range(2):
            own[h, r, i] = part(h, r, chunk_at(h, zs + i, coords[h][0]))

    def joined(h, r, i):
        copy1(h, r, zs + i).wait_recv()
        copy2(h, r, i).wait_recv()
        return (
            own[h, r, i]
            + recv1[h, r, zs + i].astype(jnp.float32)
            + recv2[h, r, i].astype(jnp.float32)
        )

    def third(r, i):
        for h in range(2):
            send3[h, r, i] = joined(h, r, i).astype(send3.dtype)
            copy3(h, r, i).start()

    def last(r):
        for h in range(2):
            own[h, r, zs - 1] = joined(h, r, zs - 1)

    def gather(q):
        back_from(q).wait_recv()
        tile = asked_ref[q]
        wide = jnp.concatenate([tile] * (BLOCK // tile.shape[0]), axis=0)
        block = came[q].astype(jnp.float32)
        for b in range(nb):
            total[b] += jnp.where(wide == b, block, 0.0)

    prepare(0, 0)
    pl.semaphore_wait(barrier, n - 1 + tp - 1)
    for h in range(2):
        copy1(h, 0, 0).start()
    loop(1, zs, lambda i: first(0, i))
    loop(0, zs, lambda i: second(0, i))
    for r in range(1, rounds):
        loop(0, zs, lambda i: first(r, i))
        if r == 1:
            loop(0, me, lambda p: back_to(p).start())

        def both(i):
            third(r - 1, i)
            second(r, i)

        loop(0, zs - 1, both)
        last(r - 1)
        second(r, zs - 1)

    total[...] = own_ref[...]
    loop(me + 1, n, gather)
    for k in range(1, tp):
        across(k).start()
    loop(0, zs - 1, lambda i: third(rounds - 1, i))
    for k in range(1, tp):
        across(k).wait_recv()
    summed = total[...]
    for k in range(1, tp):
        summed = summed + others[k - 1]
    flat = summed.reshape(nb * BLOCK, 2 * BLOCK).T
    dk_ref[...] = flat[:BLOCK]
    dv_ref[...] = flat[BLOCK:]

    def finish(r):
        def arrived(i):
            for h in range(2):
                copy3(h, r, i).wait_recv()
                own[h, r, zs - 1] += recv3[h, r, i].astype(jnp.float32)

        loop(0, zs - 1, arrived)

    for r in range(rounds - 1):
        finish(r)
    last(rounds - 1)
    finish(rounds - 1)
    whole = jnp.concatenate(
        [own[h, r, zs - 1] for r in range(rounds) for h in range(2)], axis=0
    )
    wg_ref[...] = whole.T

    for r in range(rounds):
        for h in range(2):
            loop(0, 2 * zs, lambda i: copy1(h, r, i).wait_send())
            loop(0, zs, lambda i: copy2(h, r, i).wait_send())
            loop(0, zs - 1, lambda i: copy3(h, r, i).wait_send())
    loop(0, me, lambda p: back_to(p).wait_send())
    for k in range(1, tp):
        across(k).wait_send()


def shards(n, tp, normed, queries, keys, values, attended, cotangent, log_sum, chosen):
    me = lax.axis_index("kv")
    tok_rows, model_width = normed.shape
    slot_count = chosen.shape[1]
    nb = tok_rows // BLOCK
    heads = log_sum.shape[1]
    cols = queries.shape[1]
    pair = 2 * BLOCK
    vmem = pl.BlockSpec(memory_space=pltpu.VMEM)
    dma = pltpu.SemaphoreType.DMA

    owners = chosen // nb
    within = chosen % nb
    listed = chosen >= 0
    remote = listed & (owners != me)
    peer_ids = jnp.arange(n, dtype=jnp.int32)
    matched = remote[:, :, None] & (owners[:, :, None] == peer_ids)
    wanted = jnp.max(jnp.where(matched, within[:, :, None], -1), axis=(0, 1))
    wanted = jnp.broadcast_to(wanted[:, None, None], (n, 8, 128))
    slots = jnp.where(listed, jnp.where(owners == me, within, nb + owners), 0)
    row_base = (me * nb + jnp.arange(nb, dtype=jnp.int32))[:, None]
    limits = jnp.where(listed, (chosen - row_base) * BLOCK, 4 * BLOCK)
    counts = jnp.sum(listed.astype(jnp.int32), axis=1)

    table, asked = pl.pallas_call(
        functools.partial(fetch_kernel, n, nb),
        out_shape=(
            jax.ShapeDtypeStruct((nb + n, BLOCK, pair), jnp.bfloat16),
            jax.ShapeDtypeStruct((n, 8, 128), jnp.int32),
        ),
        in_specs=[vmem] * 3,
        out_specs=(vmem, vmem),
        scratch_shapes=[pltpu.VMEM((n, BLOCK, pair), jnp.bfloat16)] + [dma((n,))] * 4,
        compiler_params=pltpu.CompilerParams(collective_id=0, has_side_effects=True),
        name="fetch",
    )(keys.T, values.T, wanted)

    logs = log_sum.reshape(nb, BLOCK, heads).transpose(0, 2, 1).reshape(nb, 1, heads * BLOCK)
    rows_spec = pl.BlockSpec((BLOCK, cols), lambda g, *_: (g, 0))
    gq, own_part, back = pl.pallas_call(
        functools.partial(attention_kernel, heads, nb, n),
        out_shape=(
            jax.ShapeDtypeStruct((tok_rows, cols), jnp.bfloat16),
            jax.ShapeDtypeStruct((nb, BLOCK, pair), jnp.float32),
            jax.ShapeDtypeStruct((n, BLOCK, pair), jnp.bfloat16),
        ),
        grid_spec=pltpu.PrefetchScalarGridSpec(
            num_scalar_prefetch=3,
            grid=(nb,),
            in_specs=[
                rows_spec,
                rows_spec,
                rows_spec,
                pl.BlockSpec((1, 1, heads * BLOCK), lambda g, *_: (g, 0, 0)),
                pl.BlockSpec((nb + n, BLOCK, pair), lambda g, *_: (0, 0, 0)),
            ],
            out_specs=(
                rows_spec,
                pl.BlockSpec((nb, BLOCK, pair), lambda g, *_: (0, 0, 0)),
                pl.BlockSpec((n, BLOCK, pair), lambda g, *_: (0, 0, 0)),
            ),
            scratch_shapes=[
                pltpu.VMEM((nb + n, BLOCK, pair), jnp.float32),
                pltpu.VMEM((BLOCK, heads * BLOCK), jnp.float32),
            ],
        ),
        compiler_params=pltpu.CompilerParams(dimension_semantics=("arbitrary",)),
        name="attention",
    )(slots, limits, counts, queries, attended, cotangent, logs, table)

    zs = n // 4
    rounds = ROUNDS
    half = cols // (2 * rounds)
    width = model_width // n
    low = jnp.bfloat16
    wide = jnp.float32
    weight_grad, grad_keys, grad_values = pl.pallas_call(
        functools.partial(reduce_kernel, n, tp, nb, rounds),
        out_shape=(
            jax.ShapeDtypeStruct((width, cols), wide),
            jax.ShapeDtypeStruct((BLOCK, tok_rows), wide),
            jax.ShapeDtypeStruct((BLOCK, tok_rows), wide),
        ),
        in_specs=[vmem] * 5,
        out_specs=(vmem, vmem, vmem),
        scratch_shapes=[
            pltpu.VMEM((2, rounds, half, tok_rows), low),
            pltpu.VMEM((2, rounds, 2 * zs, half, width), low),
            pltpu.VMEM((2, rounds, 2 * zs, half, width), low),
            pltpu.VMEM((2, rounds, zs, half, width), wide),
            pltpu.VMEM((2, rounds, zs, half, width), low),
            pltpu.VMEM((2, rounds, zs, half, width), low),
            pltpu.VMEM((2, rounds, zs - 1, half, width), low),
            pltpu.VMEM((2, rounds, zs - 1, half, width), low),
            pltpu.VMEM((n, BLOCK, pair), low),
            pltpu.VMEM((nb, BLOCK, pair), wide),
            pltpu.VMEM((tp - 1, nb, BLOCK, pair), wide),
            dma((2, rounds, 2 * zs)), dma((2, rounds, 2 * zs)),
            dma((2, rounds, zs)), dma((2, rounds, zs)),
            dma((2, rounds, zs - 1)), dma((2, rounds, zs - 1)),
            dma((n,)), dma((n,)),
            dma((tp - 1,)), dma((tp - 1,)),
        ],
        compiler_params=pltpu.CompilerParams(
            collective_id=1, has_side_effects=True, vmem_limit_bytes=56 * 1024 * 1024
        ),
        name="reduce",
    )(normed, gq, own_part, back, asked)
    return (gq, grad_keys.T, grad_values.T, weight_grad)


def solution(mesh):
    placed = (
        P("kv", None),
        P("kv", "tp"),
        P("kv", None),
        P("kv", None),
        P("kv", "tp"),
        P("kv", "tp"),
        P("kv", "tp"),
        P("kv", None),
    )
    return jax.shard_map(
        functools.partial(shards, mesh.shape["kv"], mesh.shape["tp"]),
        mesh=mesh,
        in_specs=placed,
        out_specs=(P("kv", "tp"), P("kv", None), P("kv", None), P("kv", "tp")),
        check_vma=False,
    )
```

```python
import functools

import jax
import jax.numpy as jnp
from jax import lax
from jax.experimental import pallas as pl
from jax.experimental.pallas import tpu as pltpu
from jax.sharding import PartitionSpec as P

BLOCK = 64
GROUP = 4
ROUNDS = 2
NT = (((1,), (1,)), ((), ()))
TN = (((0,), (0,)), ((), ()))


def greet(n, peers_tp):
    me = lax.axis_index("kv")
    barrier = pltpu.get_barrier_semaphore()

    def hello(k, _):
        pl.semaphore_signal(barrier, inc=1, device_id={"kv": lax.rem(me + k, n)})
        return 0

    lax.fori_loop(1, n, hello, 0)
    if peers_tp > 1:
        mine = lax.axis_index("tp")
        for k in range(1, peers_tp):
            pl.semaphore_signal(
                barrier, inc=1, device_id={"tp": lax.rem(mine + k, peers_tp)}
            )
    return barrier


def fetch_kernel(
    n, nb, keys_ref, values_ref, chosen_ref, table_ref, asked_ref, want_ref, out_buf, s1, r1, s2, r2
):
    me = lax.axis_index("kv")
    barrier = greet(n, 1)
    pairs = jnp.concatenate([keys_ref[...], values_ref[...]], axis=0).T
    for b in range(nb):
        table_ref[b] = pairs[b * BLOCK : (b + 1) * BLOCK]

    def blank(p, _):
        table_ref[nb + p] = jnp.zeros(table_ref.shape[1:], table_ref.dtype)
        return 0

    lax.fori_loop(me, n, blank, 0)

    def unasked(p, _):
        asked_ref[p] = jnp.full(asked_ref.shape[1:], -1, jnp.int32)
        return 0

    lax.fori_loop(0, me + 1, unasked, 0)
    ids = chosen_ref[...]

    def want(p, _):
        inner = ids - p * nb
        best = jnp.where((inner >= 0) & (inner < nb), inner, -1)
        best = jnp.max(jnp.max(best, axis=1, keepdims=True), axis=0, keepdims=True)
        want_ref[p] = jnp.broadcast_to(best, want_ref.shape[1:])
        return 0

    lax.fori_loop(0, me, want, 0)
    pl.semaphore_wait(barrier, n - 1)

    def request(p):
        return pltpu.make_async_remote_copy(
            src_ref=want_ref.at[p],
            dst_ref=asked_ref.at[me],
            send_sem=s1.at[p],
            recv_sem=r1.at[me],
            device_id={"kv": p},
        )

    def asked_from(q):
        return pltpu.make_async_remote_copy(
            src_ref=want_ref.at[q],
            dst_ref=asked_ref.at[q],
            send_sem=s1.at[q],
            recv_sem=r1.at[q],
            device_id={"kv": q},
        )

    def reply(q):
        return pltpu.make_async_remote_copy(
            src_ref=out_buf.at[q],
            dst_ref=table_ref.at[nb + me],
            send_sem=s2.at[q],
            recv_sem=r2.at[me],
            device_id={"kv": q},
        )

    def reply_from(p):
        return pltpu.make_async_remote_copy(
            src_ref=out_buf.at[p],
            dst_ref=table_ref.at[nb + p],
            send_sem=s2.at[p],
            recv_sem=r2.at[p],
            device_id={"kv": p},
        )

    def step(fn):
        def body(i, _):
            fn(i)
            return 0

        return body

    lax.fori_loop(0, me, step(lambda p: request(p).start()), 0)

    def answer(q):
        asked_from(q).wait_recv()
        tile = asked_ref[q]
        wide = jnp.concatenate([tile] * (BLOCK // tile.shape[0]), axis=0)
        picked = jnp.zeros(wide.shape, jnp.float32)
        for b in range(nb):
            picked = jnp.where(wide == b, table_ref[b].astype(jnp.float32), picked)
        out_buf[q] = picked.astype(out_buf.dtype)
        reply(q).start()

    lax.fori_loop(me + 1, n, step(answer), 0)
    lax.fori_loop(0, me, step(lambda p: request(p).wait_send()), 0)
    lax.fori_loop(me + 1, n, step(lambda q: reply(q).wait_send()), 0)
    lax.fori_loop(0, me, step(lambda p: reply_from(p).wait_recv()), 0)


def attention_kernel(
    heads, nb, n, chosen,
    q_ref, o_ref, g_ref, l_ref, table_ref, gq_ref, own_ref, back_ref, acc, dqt, lines,
):
    g = pl.program_id(0)
    me = lax.axis_index("kv")
    rows = heads * BLOCK
    scale = BLOCK ** (-0.5)

    @pl.when(g == 0)
    def _():
        acc[...] = jnp.zeros_like(acc)
        for b in range(nb):
            lines[b] = jnp.concatenate(
                [l_ref[h : h + 1, b * BLOCK : (b + 1) * BLOCK] for h in range(heads)], axis=1
            )

    def slot_of(c):
        inner = c - me * nb
        near = (inner >= 0) & (inner < nb)
        return jnp.where(c < 0, 0, jnp.where(near, inner, nb + c // nb))

    def limit_of(c):
        return jnp.where(c < 0, 4 * BLOCK, (c - (me * nb + g)) * BLOCK)

    def stack(ref):
        full = ref[...]
        return jnp.concatenate([full[:, h * BLOCK : (h + 1) * BLOCK] for h in range(heads)], axis=0)

    q = stack(q_ref)
    go = stack(g_ref)
    prod = go.astype(jnp.float32) * stack(o_ref).astype(jnp.float32)
    high = prod.astype(jnp.bfloat16)
    low = (prod - high.astype(jnp.float32)).astype(jnp.bfloat16)
    ones = jnp.ones((8, BLOCK), jnp.bfloat16)
    delta = (
        lax.dot_general(ones, high, NT, preferred_element_type=jnp.float32)
        + lax.dot_general(ones, low, NT, preferred_element_type=jnp.float32)
    )[0:1]
    logs = lines[g]
    ahead = (
        lax.broadcasted_iota(jnp.int32, (BLOCK, rows), 1) % BLOCK
        - lax.broadcasted_iota(jnp.int32, (BLOCK, rows), 0)
    )
    dqt[...] = jnp.zeros_like(dqt)
    for c in range(chosen.shape[1] // GROUP):

        @pl.when(chosen[g, c * GROUP] >= 0)
        def _():
            listed = [chosen[g, c * GROUP + i] for i in range(GROUP)]
            ids = [slot_of(v) for v in listed]
            pairs = jnp.concatenate([table_ref[s] for s in ids], axis=0)
            k = pairs[:, :BLOCK]
            v = pairs[:, BLOCK:]
            s = lax.dot_general(k, q, NT, preferred_element_type=jnp.float32)
            dp = lax.dot_general(v, go, NT, preferred_element_type=jnp.float32)
            e = jnp.exp(s * scale - logs)
            p = jnp.concatenate(
                [
                    jnp.where(
                        ahead >= limit_of(listed[i]), e[i * BLOCK : (i + 1) * BLOCK], 0.0
                    )
                    for i in range(GROUP)
                ],
                axis=0,
            )
            ds = (p * (dp - delta) * scale).astype(jnp.bfloat16)
            dk = jnp.dot(ds, q, preferred_element_type=jnp.float32)
            dv = jnp.dot(p.astype(jnp.bfloat16), go, preferred_element_type=jnp.float32)
            dqt[...] += lax.dot_general(k, ds, TN, preferred_element_type=jnp.float32)
            dkv = jnp.concatenate([dk, dv], axis=1)
            for i in range(GROUP):
                acc[ids[i]] += dkv[i * BLOCK : (i + 1) * BLOCK]

    dq = dqt[...].T.astype(jnp.bfloat16)
    gq_ref[...] = jnp.concatenate([dq[h * BLOCK : (h + 1) * BLOCK] for h in range(heads)], axis=1)

    @pl.when(g == nb - 1)
    def _():
        own_ref[...] = acc[:nb]
        back_ref[...] = acc[nb:].astype(back_ref.dtype)


def reduce_kernel(
    n, tp, nb, rounds, normed_ref, gq_ref, own_ref, back_ref, asked_ref,
    wgt_ref, dkv_ref,
    gqt, send1, recv1, own, send2, recv2, send3, recv3, came, total, others,
    ss1, rs1, ss2, rs2, ss3, rs3, ssb, rsb, sst, rst,
):
    me = lax.axis_index("kv")
    mine = lax.axis_index("tp")
    zs = n // 4
    x = lax.rem(me, 2)
    y = lax.rem(me // 2, 2)
    z = me // 4
    barrier = greet(n, tp)
    rows = gqt.shape[2]
    width = send1.shape[4]
    turned = gq_ref[...].T
    for r in range(rounds):
        for h in range(2):
            gqt[h, r] = turned[(2 * r + h) * rows : (2 * r + h + 1) * rows]

    def index(zz, a, b, h):
        return zz * 4 + (b * 2 + a if h == 0 else a * 2 + b)

    coords = ((x, y), (y, x))

    def chunk_at(h, i, a):
        b = coords[h][1]
        bb = jnp.where(i < zs, 1 - b, b)
        zz = lax.rem(z + 1 + lax.rem(i, zs), zs)
        return index(zz, a, bb, h)

    def part(h, r, chunk):
        cols = pl.ds(pl.multiple_of(chunk * width, 128), width)
        return jnp.dot(gqt[h, r], normed_ref[:, cols], preferred_element_type=jnp.float32)

    def copy1(h, r, i):
        a, b = coords[h]
        return pltpu.make_async_remote_copy(
            src_ref=send1.at[h, r, i], dst_ref=recv1.at[h, r, i],
            send_sem=ss1.at[h, r, i], recv_sem=rs1.at[h, r, i],
            device_id={"kv": index(z, 1 - a, b, h)},
        )

    def copy2(h, r, i):
        a, b = coords[h]
        return pltpu.make_async_remote_copy(
            src_ref=send2.at[h, r, i], dst_ref=recv2.at[h, r, i],
            send_sem=ss2.at[h, r, i], recv_sem=rs2.at[h, r, i],
            device_id={"kv": index(z, a, 1 - b, h)},
        )

    def copy3(h, r, i):
        a, b = coords[h]
        return pltpu.make_async_remote_copy(
            src_ref=send3.at[h, r, i], dst_ref=recv3.at[h, r, i],
            send_sem=ss3.at[h, r, i], recv_sem=rs3.at[h, r, i],
            device_id={"kv": index(lax.rem(z + 1 + i, zs), a, b, h)},
        )

    def back_to(p):
        return pltpu.make_async_remote_copy(
            src_ref=back_ref.at[p], dst_ref=came.at[me],
            send_sem=ssb.at[p], recv_sem=rsb.at[me], device_id={"kv": p},
        )

    def back_from(q):
        return pltpu.make_async_remote_copy(
            src_ref=back_ref.at[q], dst_ref=came.at[q],
            send_sem=ssb.at[q], recv_sem=rsb.at[q], device_id={"kv": q},
        )

    def across(k):
        return pltpu.make_async_remote_copy(
            src_ref=total, dst_ref=others.at[k - 1],
            send_sem=sst.at[k - 1], recv_sem=rst.at[k - 1],
            device_id={"tp": lax.rem(mine + k, tp)},
        )

    def loop(start, stop, fn):
        def body(i, _):
            fn(i)
            return 0

        lax.fori_loop(start, stop, body, 0)

    def prepare(r, i):
        for h in range(2):
            send1[h, r, i] = part(h, r, chunk_at(h, i, 1 - coords[h][0])).astype(send1.dtype)

    def first(r, i):
        prepare(r, i)
        for h in range(2):
            copy1(h, r, i).start()

    def second(r, i):
        for h in range(2):
            mine_here = part(h, r, chunk_at(h, i, coords[h][0]))
            copy1(h, r, i).wait_recv()
            send2[h, r, i] = (mine_here + recv1[h, r, i].astype(jnp.float32)).astype(send2.dtype)
            copy2(h, r, i).start()
        first(r, zs + i)
        for h in range(2):
            own[h, r, i] = part(h, r, chunk_at(h, zs + i, coords[h][0]))

    def joined(h, r, i):
        copy1(h, r, zs + i).wait_recv()
        copy2(h, r, i).wait_recv()
        return (
            own[h, r, i]
            + recv1[h, r, zs + i].astype(jnp.float32)
            + recv2[h, r, i].astype(jnp.float32)
        )

    def third(r, i):
        for h in range(2):
            send3[h, r, i] = joined(h, r, i).astype(send3.dtype)
            copy3(h, r, i).start()

    def last(r):
        for h in range(2):
            own[h, r, zs - 1] = joined(h, r, zs - 1)

    def gather(q):
        back_from(q).wait_recv()
        tile = asked_ref[q]
        wide = jnp.concatenate([tile] * (BLOCK // tile.shape[0]), axis=0)
        block = came[q].astype(jnp.float32)
        for b in range(nb):
            total[b] += jnp.where(wide == b, block, 0.0)

    prepare(0, 0)
    pl.semaphore_wait(barrier, n - 1 + tp - 1)
    for h in range(2):
        copy1(h, 0, 0).start()
    loop(1, zs, lambda i: first(0, i))
    loop(0, zs, lambda i: second(0, i))
    for r in range(1, rounds):
        loop(0, zs, lambda i: first(r, i))
        if r == 1:
            loop(0, me, lambda p: back_to(p).start())

        def both(i):
            third(r - 1, i)
            second(r, i)

        loop(0, zs - 1, both)
        last(r - 1)
        second(r, zs - 1)

    total[...] = own_ref[...]
    loop(me + 1, n, gather)
    for k in range(1, tp):
        across(k).start()
    loop(0, zs - 1, lambda i: third(rounds - 1, i))
    for k in range(1, tp):
        across(k).wait_recv()
    summed = total[...]
    for k in range(1, tp):
        summed = summed + others[k - 1]
    dkv_ref[...] = summed.reshape(nb * BLOCK, 2 * BLOCK)

    def finish(r):
        def arrived(i):
            for h in range(2):
                copy3(h, r, i).wait_recv()
                own[h, r, zs - 1] += recv3[h, r, i].astype(jnp.float32)

        loop(0, zs - 1, arrived)

    for r in range(rounds - 1):
        finish(r)
    last(rounds - 1)
    finish(rounds - 1)
    for r in range(rounds):
        for h in range(2):
            wgt_ref[(2 * r + h) * rows : (2 * r + h + 1) * rows] = own[h, r, zs - 1]

    for r in range(rounds):
        for h in range(2):
            loop(0, 2 * zs, lambda i: copy1(h, r, i).wait_send())
            loop(0, zs, lambda i: copy2(h, r, i).wait_send())
            loop(0, zs - 1, lambda i: copy3(h, r, i).wait_send())
    loop(0, me, lambda p: back_to(p).wait_send())
    for k in range(1, tp):
        across(k).wait_send()


def turn_kernel(wgt_ref, dkv_ref, wg_ref, dk_ref, dv_ref):
    wg_ref[...] = wgt_ref[...].T
    flat = dkv_ref[...].T
    dk_ref[...] = flat[:BLOCK]
    dv_ref[...] = flat[BLOCK:]


def shards(n, tp, normed, queries, keys, values, attended, cotangent, log_sum, chosen):
    tok_rows, model_width = normed.shape
    nb = tok_rows // BLOCK
    heads = log_sum.shape[1]
    cols = queries.shape[1]
    pair = 2 * BLOCK
    vmem = pl.BlockSpec(memory_space=pltpu.VMEM)
    dma = pltpu.SemaphoreType.DMA

    table, asked = pl.pallas_call(
        functools.partial(fetch_kernel, n, nb),
        out_shape=(
            jax.ShapeDtypeStruct((nb + n, BLOCK, pair), jnp.bfloat16),
            jax.ShapeDtypeStruct((n, 8, 128), jnp.int32),
        ),
        in_specs=[vmem] * 3,
        out_specs=(vmem, vmem),
        scratch_shapes=[
            pltpu.VMEM((n, 8, 128), jnp.int32),
            pltpu.VMEM((n, BLOCK, pair), jnp.bfloat16),
        ]
        + [dma((n,))] * 4,
        compiler_params=pltpu.CompilerParams(collective_id=0, has_side_effects=True),
        name="fetch",
    )(keys.T, values.T, chosen)

    rows_spec = pl.BlockSpec((BLOCK, cols), lambda g, *_: (g, 0))
    gq, own_part, back = pl.pallas_call(
        functools.partial(attention_kernel, heads, nb, n),
        out_shape=(
            jax.ShapeDtypeStruct((tok_rows, cols), jnp.bfloat16),
            jax.ShapeDtypeStruct((nb, BLOCK, pair), jnp.float32),
            jax.ShapeDtypeStruct((n, BLOCK, pair), jnp.bfloat16),
        ),
        grid_spec=pltpu.PrefetchScalarGridSpec(
            num_scalar_prefetch=1,
            grid=(nb,),
            in_specs=[
                rows_spec,
                rows_spec,
                rows_spec,
                pl.BlockSpec((heads, tok_rows), lambda g, *_: (0, 0)),
                pl.BlockSpec((nb + n, BLOCK, pair), lambda g, *_: (0, 0, 0)),
            ],
            out_specs=(
                rows_spec,
                pl.BlockSpec((nb, BLOCK, pair), lambda g, *_: (0, 0, 0)),
                pl.BlockSpec((n, BLOCK, pair), lambda g, *_: (0, 0, 0)),
            ),
            scratch_shapes=[
                pltpu.VMEM((nb + n, BLOCK, pair), jnp.float32),
                pltpu.VMEM((BLOCK, heads * BLOCK), jnp.float32),
                pltpu.VMEM((nb, 1, heads * BLOCK), jnp.float32),
            ],
        ),
        compiler_params=pltpu.CompilerParams(dimension_semantics=("arbitrary",)),
        name="attention",
    )(chosen, queries, attended, cotangent, log_sum.T, table)

    zs = n // 4
    rounds = ROUNDS
    half = cols // (2 * rounds)
    width = model_width // n
    low = jnp.bfloat16
    wide = jnp.float32
    turned, dkv = pl.pallas_call(
        functools.partial(reduce_kernel, n, tp, nb, rounds),
        out_shape=(
            jax.ShapeDtypeStruct((cols, width), wide),
            jax.ShapeDtypeStruct((tok_rows, pair), wide),
        ),
        in_specs=[vmem] * 5,
        out_specs=(vmem, vmem),
        scratch_shapes=[
            pltpu.VMEM((2, rounds, half, tok_rows), low),
            pltpu.VMEM((2, rounds, 2 * zs, half, width), low),
            pltpu.VMEM((2, rounds, 2 * zs, half, width), low),
            pltpu.VMEM((2, rounds, zs, half, width), wide),
            pltpu.VMEM((2, rounds, zs, half, width), low),
            pltpu.VMEM((2, rounds, zs, half, width), low),
            pltpu.VMEM((2, rounds, zs - 1, half, width), low),
            pltpu.VMEM((2, rounds, zs - 1, half, width), low),
            pltpu.VMEM((n, BLOCK, pair), low),
            pltpu.VMEM((nb, BLOCK, pair), wide),
            pltpu.VMEM((tp - 1, nb, BLOCK, pair), wide),
            dma((2, rounds, 2 * zs)), dma((2, rounds, 2 * zs)),
            dma((2, rounds, zs)), dma((2, rounds, zs)),
            dma((2, rounds, zs - 1)), dma((2, rounds, zs - 1)),
            dma((n,)), dma((n,)),
            dma((tp - 1,)), dma((tp - 1,)),
        ],
        compiler_params=pltpu.CompilerParams(
            collective_id=1, has_side_effects=True, vmem_limit_bytes=56 * 1024 * 1024
        ),
        name="reduce",
    )(normed, gq, own_part, back, asked)
    weight_grad, grad_keys, grad_values = pl.pallas_call(
        turn_kernel,
        out_shape=(
            jax.ShapeDtypeStruct((width, cols), wide),
            jax.ShapeDtypeStruct((BLOCK, tok_rows), wide),
            jax.ShapeDtypeStruct((BLOCK, tok_rows), wide),
        ),
        in_specs=[vmem] * 2,
        out_specs=(vmem, vmem, vmem),
        name="turn",
    )(turned, dkv)
    return (gq, grad_keys.T, grad_values.T, weight_grad)


def solution(mesh):
    placed = (
        P("kv", None),
        P("kv", "tp"),
        P("kv", None),
        P("kv", None),
        P("kv", "tp"),
        P("kv", "tp"),
        P("kv", "tp"),
        P("kv", None),
    )
    return jax.shard_map(
        functools.partial(shards, mesh.shape["kv"], mesh.shape["tp"]),
        mesh=mesh,
        in_specs=placed,
        out_specs=(P("kv", "tp"), P("kv", None), P("kv", None), P("kv", "tp")),
        check_vma=False,
    )
```

```python
import functools

import jax
import jax.numpy as jnp
from jax import lax
from jax.experimental import pallas as pl
from jax.experimental.pallas import tpu as pltpu
from jax.sharding import PartitionSpec as P

BLOCK = 64
GROUP = 16
ROUNDS = 2
NT = (((1,), (1,)), ((), ()))
TN = (((0,), (0,)), ((), ()))


def greet(n, peers_tp):
    me = lax.axis_index("kv")
    barrier = pltpu.get_barrier_semaphore()

    def hello(k, _):
        pl.semaphore_signal(barrier, inc=1, device_id={"kv": lax.rem(me + k, n)})
        return 0

    lax.fori_loop(1, n, hello, 0)
    if peers_tp > 1:
        mine = lax.axis_index("tp")
        for k in range(1, peers_tp):
            pl.semaphore_signal(
                barrier, inc=1, device_id={"tp": lax.rem(mine + k, peers_tp)}
            )
    return barrier


def fetch_kernel(
    n, nb, keys_ref, values_ref, chosen_ref, table_ref, asked_ref, want_ref, out_buf, s1, r1, s2, r2
):
    me = lax.axis_index("kv")
    barrier = greet(n, 1)
    pairs = jnp.concatenate([keys_ref[...], values_ref[...]], axis=0).T
    for b in range(nb):
        table_ref[b] = pairs[b * BLOCK : (b + 1) * BLOCK]

    def blank(p, _):
        table_ref[nb + p] = jnp.zeros(table_ref.shape[1:], table_ref.dtype)
        return 0

    lax.fori_loop(me, n, blank, 0)

    def unasked(p, _):
        asked_ref[p] = jnp.full(asked_ref.shape[1:], -1, jnp.int32)
        return 0

    lax.fori_loop(0, me + 1, unasked, 0)
    ids = chosen_ref[...]

    def want(p, _):
        inner = ids - p * nb
        best = jnp.where((inner >= 0) & (inner < nb), inner, -1)
        best = jnp.max(jnp.max(best, axis=1, keepdims=True), axis=0, keepdims=True)
        want_ref[p] = jnp.broadcast_to(best, want_ref.shape[1:])
        return 0

    lax.fori_loop(0, me, want, 0)
    pl.semaphore_wait(barrier, n - 1)

    def request(p):
        return pltpu.make_async_remote_copy(
            src_ref=want_ref.at[p],
            dst_ref=asked_ref.at[me],
            send_sem=s1.at[p],
            recv_sem=r1.at[me],
            device_id={"kv": p},
        )

    def asked_from(q):
        return pltpu.make_async_remote_copy(
            src_ref=want_ref.at[q],
            dst_ref=asked_ref.at[q],
            send_sem=s1.at[q],
            recv_sem=r1.at[q],
            device_id={"kv": q},
        )

    def reply(q):
        return pltpu.make_async_remote_copy(
            src_ref=out_buf.at[q],
            dst_ref=table_ref.at[nb + me],
            send_sem=s2.at[q],
            recv_sem=r2.at[me],
            device_id={"kv": q},
        )

    def reply_from(p):
        return pltpu.make_async_remote_copy(
            src_ref=out_buf.at[p],
            dst_ref=table_ref.at[nb + p],
            send_sem=s2.at[p],
            recv_sem=r2.at[p],
            device_id={"kv": p},
        )

    def step(fn):
        def body(i, _):
            fn(i)
            return 0

        return body

    lax.fori_loop(0, me, step(lambda p: request(p).start()), 0)

    def answer(q):
        asked_from(q).wait_recv()
        tile = asked_ref[q]
        wide = jnp.concatenate([tile] * (BLOCK // tile.shape[0]), axis=0)
        picked = jnp.zeros(wide.shape, jnp.float32)
        for b in range(nb):
            picked = jnp.where(wide == b, table_ref[b].astype(jnp.float32), picked)
        out_buf[q] = picked.astype(out_buf.dtype)
        reply(q).start()

    lax.fori_loop(me + 1, n, step(answer), 0)
    lax.fori_loop(0, me, step(lambda p: request(p).wait_send()), 0)
    lax.fori_loop(me + 1, n, step(lambda q: reply(q).wait_send()), 0)
    lax.fori_loop(0, me, step(lambda p: reply_from(p).wait_recv()), 0)


def attention_kernel(
    heads, nb, n, chosen,
    q_ref, o_ref, g_ref, l_ref, table_ref, gq_ref, own_ref, back_ref, acc, dqt, lines,
):
    g = pl.program_id(0)
    me = lax.axis_index("kv")
    rows = heads * BLOCK
    scale = BLOCK ** (-0.5)

    @pl.when(g == 0)
    def _():
        acc[...] = jnp.zeros_like(acc)
        for b in range(nb):
            lines[b] = jnp.concatenate(
                [l_ref[h : h + 1, b * BLOCK : (b + 1) * BLOCK] for h in range(heads)], axis=1
            )

    def slot_of(c):
        inner = c - me * nb
        near = (inner >= 0) & (inner < nb)
        return jnp.where(c < 0, 0, jnp.where(near, inner, nb + c // nb))

    def limit_of(c):
        return jnp.where(c < 0, 4 * BLOCK, (c - (me * nb + g)) * BLOCK)

    def stack(ref):
        full = ref[...]
        return jnp.concatenate([full[:, h * BLOCK : (h + 1) * BLOCK] for h in range(heads)], axis=0)

    q = stack(q_ref)
    go = stack(g_ref)
    prod = go.astype(jnp.float32) * stack(o_ref).astype(jnp.float32)
    high = prod.astype(jnp.bfloat16)
    low = (prod - high.astype(jnp.float32)).astype(jnp.bfloat16)
    ones = jnp.ones((8, BLOCK), jnp.bfloat16)
    delta = (
        lax.dot_general(ones, high, NT, preferred_element_type=jnp.float32)
        + lax.dot_general(ones, low, NT, preferred_element_type=jnp.float32)
    )[0:1]
    logs = lines[g]
    ahead = (
        lax.broadcasted_iota(jnp.int32, (BLOCK, rows), 1) % BLOCK
        - lax.broadcasted_iota(jnp.int32, (BLOCK, rows), 0)
    )
    dqt[...] = jnp.zeros_like(dqt)
    for c in range(chosen.shape[1] // GROUP):

        @pl.when(chosen[g, c * GROUP] >= 0)
        def _():
            listed = [chosen[g, c * GROUP + i] for i in range(GROUP)]
            ids = [slot_of(v) for v in listed]
            pairs = jnp.concatenate([table_ref[s] for s in ids], axis=0)
            k = pairs[:, :BLOCK]
            v = pairs[:, BLOCK:]
            s = lax.dot_general(k, q, NT, preferred_element_type=jnp.float32)
            dp = lax.dot_general(v, go, NT, preferred_element_type=jnp.float32)
            e = jnp.exp(s * scale - logs)
            p = jnp.concatenate(
                [
                    jnp.where(
                        ahead >= limit_of(listed[i]), e[i * BLOCK : (i + 1) * BLOCK], 0.0
                    )
                    for i in range(GROUP)
                ],
                axis=0,
            )
            ds = (p * (dp - delta) * scale).astype(jnp.bfloat16)
            dk = jnp.dot(ds, q, preferred_element_type=jnp.float32)
            dv = jnp.dot(p.astype(jnp.bfloat16), go, preferred_element_type=jnp.float32)
            dqt[...] += lax.dot_general(k, ds, TN, preferred_element_type=jnp.float32)
            dkv = jnp.concatenate([dk, dv], axis=1)
            for i in range(GROUP):
                acc[ids[i]] += dkv[i * BLOCK : (i + 1) * BLOCK]

    dq = dqt[...].T.astype(jnp.bfloat16)
    gq_ref[...] = jnp.concatenate([dq[h * BLOCK : (h + 1) * BLOCK] for h in range(heads)], axis=1)

    @pl.when(g == nb - 1)
    def _():
        own_ref[...] = acc[:nb]
        back_ref[...] = acc[nb:].astype(back_ref.dtype)


def reduce_kernel(
    n, tp, nb, rounds, normed_ref, gq_ref, own_ref, back_ref, asked_ref,
    wgt_ref, dkv_ref,
    gqt, send1, recv1, own, send2, recv2, send3, recv3, came, total, others,
    ss1, rs1, ss2, rs2, ss3, rs3, ssb, rsb, sst, rst,
):
    me = lax.axis_index("kv")
    mine = lax.axis_index("tp")
    zs = n // 4
    x = lax.rem(me, 2)
    y = lax.rem(me // 2, 2)
    z = me // 4
    barrier = greet(n, tp)
    rows = gqt.shape[2]
    width = send1.shape[4]
    turned = gq_ref[...].T
    for r in range(rounds):
        for h in range(2):
            gqt[h, r] = turned[(2 * r + h) * rows : (2 * r + h + 1) * rows]

    def index(zz, a, b, h):
        return zz * 4 + (b * 2 + a if h == 0 else a * 2 + b)

    coords = ((x, y), (y, x))

    def chunk_at(h, i, a):
        b = coords[h][1]
        bb = jnp.where(i < zs, 1 - b, b)
        zz = lax.rem(z + 1 + lax.rem(i, zs), zs)
        return index(zz, a, bb, h)

    def part(h, r, chunk):
        cols = pl.ds(pl.multiple_of(chunk * width, 128), width)
        return jnp.dot(gqt[h, r], normed_ref[:, cols], preferred_element_type=jnp.float32)

    def copy1(h, r, i):
        a, b = coords[h]
        return pltpu.make_async_remote_copy(
            src_ref=send1.at[h, r, i], dst_ref=recv1.at[h, r, i],
            send_sem=ss1.at[h, r, i], recv_sem=rs1.at[h, r, i],
            device_id={"kv": index(z, 1 - a, b, h)},
        )

    def copy2(h, r, i):
        a, b = coords[h]
        return pltpu.make_async_remote_copy(
            src_ref=send2.at[h, r, i], dst_ref=recv2.at[h, r, i],
            send_sem=ss2.at[h, r, i], recv_sem=rs2.at[h, r, i],
            device_id={"kv": index(z, a, 1 - b, h)},
        )

    def copy3(h, r, i):
        a, b = coords[h]
        return pltpu.make_async_remote_copy(
            src_ref=send3.at[h, r, i], dst_ref=recv3.at[h, r, i],
            send_sem=ss3.at[h, r, i], recv_sem=rs3.at[h, r, i],
            device_id={"kv": index(lax.rem(z + 1 + i, zs), a, b, h)},
        )

    def back_to(p):
        return pltpu.make_async_remote_copy(
            src_ref=back_ref.at[p], dst_ref=came.at[me],
            send_sem=ssb.at[p], recv_sem=rsb.at[me], device_id={"kv": p},
        )

    def back_from(q):
        return pltpu.make_async_remote_copy(
            src_ref=back_ref.at[q], dst_ref=came.at[q],
            send_sem=ssb.at[q], recv_sem=rsb.at[q], device_id={"kv": q},
        )

    def across(k):
        return pltpu.make_async_remote_copy(
            src_ref=total, dst_ref=others.at[k - 1],
            send_sem=sst.at[k - 1], recv_sem=rst.at[k - 1],
            device_id={"tp": lax.rem(mine + k, tp)},
        )

    def loop(start, stop, fn):
        def body(i, _):
            fn(i)
            return 0

        lax.fori_loop(start, stop, body, 0)

    def prepare(r, i):
        for h in range(2):
            send1[h, r, i] = part(h, r, chunk_at(h, i, 1 - coords[h][0])).astype(send1.dtype)

    def first(r, i):
        prepare(r, i)
        for h in range(2):
            copy1(h, r, i).start()

    def second(r, i):
        for h in range(2):
            mine_here = part(h, r, chunk_at(h, i, coords[h][0]))
            copy1(h, r, i).wait_recv()
            send2[h, r, i] = (mine_here + recv1[h, r, i].astype(jnp.float32)).astype(send2.dtype)
            copy2(h, r, i).start()
        first(r, zs + i)
        for h in range(2):
            own[h, r, i] = part(h, r, chunk_at(h, zs + i, coords[h][0]))

    def joined(h, r, i):
        copy1(h, r, zs + i).wait_recv()
        copy2(h, r, i).wait_recv()
        return (
            own[h, r, i]
            + recv1[h, r, zs + i].astype(jnp.float32)
            + recv2[h, r, i].astype(jnp.float32)
        )

    def third(r, i):
        for h in range(2):
            send3[h, r, i] = joined(h, r, i).astype(send3.dtype)
            copy3(h, r, i).start()

    def last(r):
        for h in range(2):
            own[h, r, zs - 1] = joined(h, r, zs - 1)

    def gather(q):
        back_from(q).wait_recv()
        tile = asked_ref[q]
        wide = jnp.concatenate([tile] * (BLOCK // tile.shape[0]), axis=0)
        block = came[q].astype(jnp.float32)
        for b in range(nb):
            total[b] += jnp.where(wide == b, block, 0.0)

    prepare(0, 0)
    pl.semaphore_wait(barrier, n - 1 + tp - 1)
    for h in range(2):
        copy1(h, 0, 0).start()
    loop(1, zs, lambda i: first(0, i))
    loop(0, zs, lambda i: second(0, i))
    for r in range(1, rounds):
        loop(0, zs, lambda i: first(r, i))
        if r == 1:
            loop(0, me, lambda p: back_to(p).start())

        def both(i):
            third(r - 1, i)
            second(r, i)

        loop(0, zs - 1, both)
        last(r - 1)
        second(r, zs - 1)

    total[...] = own_ref[...]
    loop(me + 1, n, gather)
    for k in range(1, tp):
        across(k).start()
    loop(0, zs - 1, lambda i: third(rounds - 1, i))
    for k in range(1, tp):
        across(k).wait_recv()
    summed = total[...]
    for k in range(1, tp):
        summed = summed + others[k - 1]
    dkv_ref[...] = summed.reshape(nb * BLOCK, 2 * BLOCK)

    def finish(r):
        def arrived(i):
            for h in range(2):
                copy3(h, r, i).wait_recv()
                own[h, r, zs - 1] += recv3[h, r, i].astype(jnp.float32)

        loop(0, zs - 1, arrived)

    for r in range(rounds - 1):
        finish(r)
    last(rounds - 1)
    finish(rounds - 1)
    for r in range(rounds):
        for h in range(2):
            wgt_ref[(2 * r + h) * rows : (2 * r + h + 1) * rows] = own[h, r, zs - 1]

    for r in range(rounds):
        for h in range(2):
            loop(0, 2 * zs, lambda i: copy1(h, r, i).wait_send())
            loop(0, zs, lambda i: copy2(h, r, i).wait_send())
            loop(0, zs - 1, lambda i: copy3(h, r, i).wait_send())
    loop(0, me, lambda p: back_to(p).wait_send())
    for k in range(1, tp):
        across(k).wait_send()


def turn_kernel(wgt_ref, dkv_ref, wg_ref, dk_ref, dv_ref):
    wg_ref[...] = wgt_ref[...].T
    flat = dkv_ref[...].T
    dk_ref[...] = flat[:BLOCK]
    dv_ref[...] = flat[BLOCK:]


def shards(n, tp, normed, queries, keys, values, attended, cotangent, log_sum, chosen):
    tok_rows, model_width = normed.shape
    nb = tok_rows // BLOCK
    heads = log_sum.shape[1]
    cols = queries.shape[1]
    pair = 2 * BLOCK
    vmem = pl.BlockSpec(memory_space=pltpu.VMEM)
    dma = pltpu.SemaphoreType.DMA

    table, asked = pl.pallas_call(
        functools.partial(fetch_kernel, n, nb),
        out_shape=(
            jax.ShapeDtypeStruct((nb + n, BLOCK, pair), jnp.bfloat16),
            jax.ShapeDtypeStruct((n, 8, 128), jnp.int32),
        ),
        in_specs=[vmem] * 3,
        out_specs=(vmem, vmem),
        scratch_shapes=[
            pltpu.VMEM((n, 8, 128), jnp.int32),
            pltpu.VMEM((n, BLOCK, pair), jnp.bfloat16),
        ]
        + [dma((n,))] * 4,
        compiler_params=pltpu.CompilerParams(collective_id=0, has_side_effects=True),
        name="fetch",
    )(keys.T, values.T, chosen)

    rows_spec = pl.BlockSpec((BLOCK, cols), lambda g, *_: (g, 0))
    gq, own_part, back = pl.pallas_call(
        functools.partial(attention_kernel, heads, nb, n),
        out_shape=(
            jax.ShapeDtypeStruct((tok_rows, cols), jnp.bfloat16),
            jax.ShapeDtypeStruct((nb, BLOCK, pair), jnp.float32),
            jax.ShapeDtypeStruct((n, BLOCK, pair), jnp.bfloat16),
        ),
        grid_spec=pltpu.PrefetchScalarGridSpec(
            num_scalar_prefetch=1,
            grid=(nb,),
            in_specs=[
                rows_spec,
                rows_spec,
                rows_spec,
                pl.BlockSpec((heads, tok_rows), lambda g, *_: (0, 0)),
                pl.BlockSpec((nb + n, BLOCK, pair), lambda g, *_: (0, 0, 0)),
            ],
            out_specs=(
                rows_spec,
                pl.BlockSpec((nb, BLOCK, pair), lambda g, *_: (0, 0, 0)),
                pl.BlockSpec((n, BLOCK, pair), lambda g, *_: (0, 0, 0)),
            ),
            scratch_shapes=[
                pltpu.VMEM((nb + n, BLOCK, pair), jnp.float32),
                pltpu.VMEM((BLOCK, heads * BLOCK), jnp.float32),
                pltpu.VMEM((nb, 1, heads * BLOCK), jnp.float32),
            ],
        ),
        compiler_params=pltpu.CompilerParams(dimension_semantics=("arbitrary",)),
        name="attention",
    )(chosen, queries, attended, cotangent, log_sum.T, table)

    zs = n // 4
    rounds = ROUNDS
    half = cols // (2 * rounds)
    width = model_width // n
    low = jnp.bfloat16
    wide = jnp.float32
    turned, dkv = pl.pallas_call(
        functools.partial(reduce_kernel, n, tp, nb, rounds),
        out_shape=(
            jax.ShapeDtypeStruct((cols, width), wide),
            jax.ShapeDtypeStruct((tok_rows, pair), wide),
        ),
        in_specs=[vmem] * 5,
        out_specs=(vmem, vmem),
        scratch_shapes=[
            pltpu.VMEM((2, rounds, half, tok_rows), low),
            pltpu.VMEM((2, rounds, 2 * zs, half, width), low),
            pltpu.VMEM((2, rounds, 2 * zs, half, width), low),
            pltpu.VMEM((2, rounds, zs, half, width), wide),
            pltpu.VMEM((2, rounds, zs, half, width), low),
            pltpu.VMEM((2, rounds, zs, half, width), low),
            pltpu.VMEM((2, rounds, zs - 1, half, width), low),
            pltpu.VMEM((2, rounds, zs - 1, half, width), low),
            pltpu.VMEM((n, BLOCK, pair), low),
            pltpu.VMEM((nb, BLOCK, pair), wide),
            pltpu.VMEM((tp - 1, nb, BLOCK, pair), wide),
            dma((2, rounds, 2 * zs)), dma((2, rounds, 2 * zs)),
            dma((2, rounds, zs)), dma((2, rounds, zs)),
            dma((2, rounds, zs - 1)), dma((2, rounds, zs - 1)),
            dma((n,)), dma((n,)),
            dma((tp - 1,)), dma((tp - 1,)),
        ],
        compiler_params=pltpu.CompilerParams(
            collective_id=1, has_side_effects=True, vmem_limit_bytes=56 * 1024 * 1024
        ),
        name="reduce",
    )(normed, gq, own_part, back, asked)
    weight_grad, grad_keys, grad_values = pl.pallas_call(
        turn_kernel,
        out_shape=(
            jax.ShapeDtypeStruct((width, cols), wide),
            jax.ShapeDtypeStruct((BLOCK, tok_rows), wide),
            jax.ShapeDtypeStruct((BLOCK, tok_rows), wide),
        ),
        in_specs=[vmem] * 2,
        out_specs=(vmem, vmem, vmem),
        name="turn",
    )(turned, dkv)
    return (gq, grad_keys.T, grad_values.T, weight_grad)


def solution(mesh):
    placed = (
        P("kv", None),
        P("kv", "tp"),
        P("kv", None),
        P("kv", None),
        P("kv", "tp"),
        P("kv", "tp"),
        P("kv", "tp"),
        P("kv", None),
    )
    return jax.shard_map(
        functools.partial(shards, mesh.shape["kv"], mesh.shape["tp"]),
        mesh=mesh,
        in_specs=placed,
        out_specs=(P("kv", "tp"), P("kv", None), P("kv", None), P("kv", "tp")),
        check_vma=False,
    )
```

```python
import functools

import jax
import jax.numpy as jnp
from jax import lax
from jax.experimental import pallas as pl
from jax.experimental.pallas import tpu as pltpu
from jax.sharding import PartitionSpec as P

BLOCK = 64
GROUP = 16
ROUNDS = 2
NT = (((1,), (1,)), ((), ()))
TN = (((0,), (0,)), ((), ()))


def greet(n, peers_tp):
    me = lax.axis_index("kv")
    barrier = pltpu.get_barrier_semaphore()

    def hello(k, _):
        pl.semaphore_signal(barrier, inc=1, device_id={"kv": lax.rem(me + k, n)})
        return 0

    lax.fori_loop(1, n, hello, 0)
    if peers_tp > 1:
        mine = lax.axis_index("tp")
        for k in range(1, peers_tp):
            pl.semaphore_signal(
                barrier, inc=1, device_id={"tp": lax.rem(mine + k, peers_tp)}
            )
    return barrier


def fetch_kernel(
    n, nb, keys_ref, values_ref, chosen_ref, table_ref, asked_ref, want_ref, out_buf, s1, r1, s2, r2
):
    me = lax.axis_index("kv")
    barrier = greet(n, 1)
    pairs = jnp.concatenate([keys_ref[...], values_ref[...]], axis=0).T
    for b in range(nb):
        table_ref[b] = pairs[b * BLOCK : (b + 1) * BLOCK]

    def blank(p, _):
        table_ref[nb + p] = jnp.zeros(table_ref.shape[1:], table_ref.dtype)
        return 0

    lax.fori_loop(me, n, blank, 0)

    def unasked(p, _):
        asked_ref[p] = jnp.full(asked_ref.shape[1:], -1, jnp.int32)
        return 0

    lax.fori_loop(0, me + 1, unasked, 0)
    ids = chosen_ref[...]

    def want(p, _):
        inner = ids - p * nb
        best = jnp.where((inner >= 0) & (inner < nb), inner, -1)
        best = jnp.max(jnp.max(best, axis=1, keepdims=True), axis=0, keepdims=True)
        want_ref[p] = jnp.broadcast_to(best, want_ref.shape[1:])
        return 0

    lax.fori_loop(0, me, want, 0)
    pl.semaphore_wait(barrier, n - 1)

    def request(p):
        return pltpu.make_async_remote_copy(
            src_ref=want_ref.at[p],
            dst_ref=asked_ref.at[me],
            send_sem=s1.at[p],
            recv_sem=r1.at[me],
            device_id={"kv": p},
        )

    def asked_from(q):
        return pltpu.make_async_remote_copy(
            src_ref=want_ref.at[q],
            dst_ref=asked_ref.at[q],
            send_sem=s1.at[q],
            recv_sem=r1.at[q],
            device_id={"kv": q},
        )

    def reply(q):
        return pltpu.make_async_remote_copy(
            src_ref=out_buf.at[q],
            dst_ref=table_ref.at[nb + me],
            send_sem=s2.at[q],
            recv_sem=r2.at[me],
            device_id={"kv": q},
        )

    def reply_from(p):
        return pltpu.make_async_remote_copy(
            src_ref=out_buf.at[p],
            dst_ref=table_ref.at[nb + p],
            send_sem=s2.at[p],
            recv_sem=r2.at[p],
            device_id={"kv": p},
        )

    def step(fn):
        def body(i, _):
            fn(i)
            return 0

        return body

    lax.fori_loop(0, me, step(lambda p: request(p).start()), 0)

    def answer(q):
        asked_from(q).wait_recv()
        tile = asked_ref[q]
        wide = jnp.concatenate([tile] * (BLOCK // tile.shape[0]), axis=0)
        picked = jnp.zeros(wide.shape, jnp.float32)
        for b in range(nb):
            picked = jnp.where(wide == b, table_ref[b].astype(jnp.float32), picked)
        out_buf[q] = picked.astype(out_buf.dtype)
        reply(q).start()

    lax.fori_loop(me + 1, n, step(answer), 0)
    lax.fori_loop(0, me, step(lambda p: request(p).wait_send()), 0)
    lax.fori_loop(me + 1, n, step(lambda q: reply(q).wait_send()), 0)
    lax.fori_loop(0, me, step(lambda p: reply_from(p).wait_recv()), 0)


def attention_kernel(
    heads, nb, n, chosen,
    q_ref, o_ref, g_ref, l_ref, table_ref, gq_ref, own_ref, back_ref, acc, dqt, lines,
):
    g = pl.program_id(0)
    me = lax.axis_index("kv")
    rows = heads * BLOCK
    scale = BLOCK ** (-0.5)

    @pl.when(g == 0)
    def _():
        acc[...] = jnp.zeros_like(acc)
        for b in range(nb):
            lines[b] = jnp.concatenate(
                [l_ref[h : h + 1, b * BLOCK : (b + 1) * BLOCK] for h in range(heads)], axis=1
            )

    def slot_of(c):
        inner = c - me * nb
        near = (inner >= 0) & (inner < nb)
        return jnp.where(c < 0, 0, jnp.where(near, inner, nb + c // nb))

    def limit_of(c):
        return jnp.where(c < 0, 4 * BLOCK, (c - (me * nb + g)) * BLOCK)

    def stack(ref):
        full = ref[...]
        return jnp.concatenate([full[:, h * BLOCK : (h + 1) * BLOCK] for h in range(heads)], axis=0)

    q = stack(q_ref) * jnp.bfloat16(scale)
    go = stack(g_ref)
    prod = go.astype(jnp.float32) * stack(o_ref).astype(jnp.float32)
    high = prod.astype(jnp.bfloat16)
    low = (prod - high.astype(jnp.float32)).astype(jnp.bfloat16)
    ones = jnp.ones((8, BLOCK), jnp.bfloat16)
    delta = (
        lax.dot_general(ones, high, NT, preferred_element_type=jnp.float32)
        + lax.dot_general(ones, low, NT, preferred_element_type=jnp.float32)
    )[0:1]
    logs = lines[g]
    ahead = (
        lax.broadcasted_iota(jnp.int32, (BLOCK, rows), 1) % BLOCK
        - lax.broadcasted_iota(jnp.int32, (BLOCK, rows), 0)
    )
    dqt[...] = jnp.zeros_like(dqt)
    for c in range(chosen.shape[1] // GROUP):

        @pl.when(chosen[g, c * GROUP] >= 0)
        def _():
            listed = [chosen[g, c * GROUP + i] for i in range(GROUP)]
            ids = [slot_of(v) for v in listed]
            pairs = jnp.concatenate([table_ref[s] for s in ids], axis=0)
            k = pairs[:, :BLOCK]
            v = pairs[:, BLOCK:]
            s = lax.dot_general(k, q, NT, preferred_element_type=jnp.float32)
            dp = lax.dot_general(v, go, NT, preferred_element_type=jnp.float32)
            e = jnp.exp(s - logs)
            p = jnp.concatenate(
                [
                    jnp.where(
                        ahead >= limit_of(listed[i]), e[i * BLOCK : (i + 1) * BLOCK], 0.0
                    )
                    for i in range(GROUP)
                ],
                axis=0,
            )
            ds = (p * (dp - delta)).astype(jnp.bfloat16)
            dk = jnp.dot(ds, q, preferred_element_type=jnp.float32)
            dv = jnp.dot(p.astype(jnp.bfloat16), go, preferred_element_type=jnp.float32)
            dqt[...] += lax.dot_general(k, ds, TN, preferred_element_type=jnp.float32)
            dkv = jnp.concatenate([dk, dv], axis=1)
            for i in range(GROUP):
                acc[ids[i]] += dkv[i * BLOCK : (i + 1) * BLOCK]

    dq = (dqt[...] * scale).T.astype(jnp.bfloat16)
    gq_ref[...] = jnp.concatenate([dq[h * BLOCK : (h + 1) * BLOCK] for h in range(heads)], axis=1)

    @pl.when(g == nb - 1)
    def _():
        own_ref[...] = acc[:nb]
        back_ref[...] = acc[nb:].astype(back_ref.dtype)


def reduce_kernel(
    n, tp, nb, rounds, normed_hbm, gq_ref, own_ref, back_ref, asked_ref,
    wgt_ref, dkv_ref,
    gqt, send1, recv1, own, send2, recv2, send3, recv3, came, total, others,
    ss1, rs1, ss2, rs2, ss3, rs3, ssb, rsb, sst, rst, normed_ref, load_sem,
):
    me = lax.axis_index("kv")
    mine = lax.axis_index("tp")
    zs = n // 4
    x = lax.rem(me, 2)
    y = lax.rem(me // 2, 2)
    z = me // 4
    load = pltpu.make_async_copy(normed_hbm, normed_ref, load_sem)
    load.start()
    barrier = greet(n, tp)
    rows = gqt.shape[2]
    width = send1.shape[4]
    turned = gq_ref[...].T
    for r in range(rounds):
        for h in range(2):
            gqt[h, r] = turned[(2 * r + h) * rows : (2 * r + h + 1) * rows]

    def index(zz, a, b, h):
        return zz * 4 + (b * 2 + a if h == 0 else a * 2 + b)

    coords = ((x, y), (y, x))

    def chunk_at(h, i, a):
        b = coords[h][1]
        bb = jnp.where(i < zs, 1 - b, b)
        zz = lax.rem(z + 1 + lax.rem(i, zs), zs)
        return index(zz, a, bb, h)

    def part(h, r, chunk):
        cols = pl.ds(pl.multiple_of(chunk * width, 128), width)
        return jnp.dot(gqt[h, r], normed_ref[:, cols], preferred_element_type=jnp.float32)

    def copy1(h, r, i):
        a, b = coords[h]
        return pltpu.make_async_remote_copy(
            src_ref=send1.at[h, r, i], dst_ref=recv1.at[h, r, i],
            send_sem=ss1.at[h, r, i], recv_sem=rs1.at[h, r, i],
            device_id={"kv": index(z, 1 - a, b, h)},
        )

    def copy2(h, r, i):
        a, b = coords[h]
        return pltpu.make_async_remote_copy(
            src_ref=send2.at[h, r, i], dst_ref=recv2.at[h, r, i],
            send_sem=ss2.at[h, r, i], recv_sem=rs2.at[h, r, i],
            device_id={"kv": index(z, a, 1 - b, h)},
        )

    def copy3(h, r, i):
        a, b = coords[h]
        return pltpu.make_async_remote_copy(
            src_ref=send3.at[h, r, i], dst_ref=recv3.at[h, r, i],
            send_sem=ss3.at[h, r, i], recv_sem=rs3.at[h, r, i],
            device_id={"kv": index(lax.rem(z + 1 + i, zs), a, b, h)},
        )

    def back_to(p):
        return pltpu.make_async_remote_copy(
            src_ref=back_ref.at[p], dst_ref=came.at[me],
            send_sem=ssb.at[p], recv_sem=rsb.at[me], device_id={"kv": p},
        )

    def back_from(q):
        return pltpu.make_async_remote_copy(
            src_ref=back_ref.at[q], dst_ref=came.at[q],
            send_sem=ssb.at[q], recv_sem=rsb.at[q], device_id={"kv": q},
        )

    def across(k):
        return pltpu.make_async_remote_copy(
            src_ref=total, dst_ref=others.at[k - 1],
            send_sem=sst.at[k - 1], recv_sem=rst.at[k - 1],
            device_id={"tp": lax.rem(mine + k, tp)},
        )

    def loop(start, stop, fn):
        def body(i, _):
            fn(i)
            return 0

        lax.fori_loop(start, stop, body, 0)

    def prepare(r, i):
        for h in range(2):
            send1[h, r, i] = part(h, r, chunk_at(h, i, 1 - coords[h][0])).astype(send1.dtype)

    def first(r, i):
        prepare(r, i)
        for h in range(2):
            copy1(h, r, i).start()

    def second(r, i):
        for h in range(2):
            mine_here = part(h, r, chunk_at(h, i, coords[h][0]))
            copy1(h, r, i).wait_recv()
            send2[h, r, i] = (mine_here + recv1[h, r, i].astype(jnp.float32)).astype(send2.dtype)
            copy2(h, r, i).start()
        first(r, zs + i)
        for h in range(2):
            own[h, r, i] = part(h, r, chunk_at(h, zs + i, coords[h][0]))

    def joined(h, r, i):
        copy1(h, r, zs + i).wait_recv()
        copy2(h, r, i).wait_recv()
        return (
            own[h, r, i]
            + recv1[h, r, zs + i].astype(jnp.float32)
            + recv2[h, r, i].astype(jnp.float32)
        )

    def third(r, i):
        for h in range(2):
            send3[h, r, i] = joined(h, r, i).astype(send3.dtype)
            copy3(h, r, i).start()

    def last(r):
        for h in range(2):
            own[h, r, zs - 1] = joined(h, r, zs - 1)

    def gather(q):
        back_from(q).wait_recv()
        tile = asked_ref[q]
        wide = jnp.concatenate([tile] * (BLOCK // tile.shape[0]), axis=0)
        block = came[q].astype(jnp.float32)
        for b in range(nb):
            total[b] += jnp.where(wide == b, block, 0.0)

    load.wait()
    prepare(0, 0)
    pl.semaphore_wait(barrier, n - 1 + tp - 1)
    for h in range(2):
        copy1(h, 0, 0).start()
    loop(1, zs, lambda i: first(0, i))
    loop(0, zs, lambda i: second(0, i))
    for r in range(1, rounds):
        loop(0, zs, lambda i: first(r, i))
        if r == 1:
            loop(0, me, lambda p: back_to(p).start())

        def both(i):
            third(r - 1, i)
            second(r, i)

        loop(0, zs - 1, both)
        last(r - 1)
        second(r, zs - 1)

    total[...] = own_ref[...]
    loop(me + 1, n, gather)
    for k in range(1, tp):
        across(k).start()
    loop(0, zs - 1, lambda i: third(rounds - 1, i))
    for k in range(1, tp):
        across(k).wait_recv()
    summed = total[...]
    for k in range(1, tp):
        summed = summed + others[k - 1]
    dkv_ref[...] = summed.reshape(nb * BLOCK, 2 * BLOCK)

    def finish(r):
        def arrived(i):
            for h in range(2):
                copy3(h, r, i).wait_recv()
                own[h, r, zs - 1] += recv3[h, r, i].astype(jnp.float32)

        loop(0, zs - 1, arrived)

    for r in range(rounds - 1):
        finish(r)
    last(rounds - 1)
    finish(rounds - 1)
    for r in range(rounds):
        for h in range(2):
            wgt_ref[(2 * r + h) * rows : (2 * r + h + 1) * rows] = own[h, r, zs - 1]

    for r in range(rounds):
        for h in range(2):
            loop(0, 2 * zs, lambda i: copy1(h, r, i).wait_send())
            loop(0, zs, lambda i: copy2(h, r, i).wait_send())
            loop(0, zs - 1, lambda i: copy3(h, r, i).wait_send())
    loop(0, me, lambda p: back_to(p).wait_send())
    for k in range(1, tp):
        across(k).wait_send()


def turn_kernel(wgt_ref, dkv_ref, wg_ref, dk_ref, dv_ref):
    wg_ref[...] = wgt_ref[...].T
    flat = dkv_ref[...].T
    dk_ref[...] = flat[:BLOCK]
    dv_ref[...] = flat[BLOCK:]


def shards(n, tp, normed, queries, keys, values, attended, cotangent, log_sum, chosen):
    tok_rows, model_width = normed.shape
    nb = tok_rows // BLOCK
    heads = log_sum.shape[1]
    cols = queries.shape[1]
    pair = 2 * BLOCK
    vmem = pl.BlockSpec(memory_space=pltpu.VMEM)
    dma = pltpu.SemaphoreType.DMA

    table, asked = pl.pallas_call(
        functools.partial(fetch_kernel, n, nb),
        out_shape=(
            jax.ShapeDtypeStruct((nb + n, BLOCK, pair), jnp.bfloat16),
            jax.ShapeDtypeStruct((n, 8, 128), jnp.int32),
        ),
        in_specs=[vmem] * 3,
        out_specs=(vmem, vmem),
        scratch_shapes=[
            pltpu.VMEM((n, 8, 128), jnp.int32),
            pltpu.VMEM((n, BLOCK, pair), jnp.bfloat16),
        ]
        + [dma((n,))] * 4,
        compiler_params=pltpu.CompilerParams(collective_id=0, has_side_effects=True),
        name="fetch",
    )(keys.T, values.T, chosen)

    rows_spec = pl.BlockSpec((BLOCK, cols), lambda g, *_: (g, 0))
    gq, own_part, back = pl.pallas_call(
        functools.partial(attention_kernel, heads, nb, n),
        out_shape=(
            jax.ShapeDtypeStruct((tok_rows, cols), jnp.bfloat16),
            jax.ShapeDtypeStruct((nb, BLOCK, pair), jnp.float32),
            jax.ShapeDtypeStruct((n, BLOCK, pair), jnp.bfloat16),
        ),
        grid_spec=pltpu.PrefetchScalarGridSpec(
            num_scalar_prefetch=1,
            grid=(nb,),
            in_specs=[
                rows_spec,
                rows_spec,
                rows_spec,
                pl.BlockSpec((heads, tok_rows), lambda g, *_: (0, 0)),
                pl.BlockSpec((nb + n, BLOCK, pair), lambda g, *_: (0, 0, 0)),
            ],
            out_specs=(
                rows_spec,
                pl.BlockSpec((nb, BLOCK, pair), lambda g, *_: (0, 0, 0)),
                pl.BlockSpec((n, BLOCK, pair), lambda g, *_: (0, 0, 0)),
            ),
            scratch_shapes=[
                pltpu.VMEM((nb + n, BLOCK, pair), jnp.float32),
                pltpu.VMEM((BLOCK, heads * BLOCK), jnp.float32),
                pltpu.VMEM((nb, 1, heads * BLOCK), jnp.float32),
            ],
        ),
        compiler_params=pltpu.CompilerParams(dimension_semantics=("arbitrary",)),
        name="attention",
    )(chosen, queries, attended, cotangent, log_sum.T, table)

    zs = n // 4
    rounds = ROUNDS
    half = cols // (2 * rounds)
    width = model_width // n
    low = jnp.bfloat16
    wide = jnp.float32
    turned, dkv = pl.pallas_call(
        functools.partial(reduce_kernel, n, tp, nb, rounds),
        out_shape=(
            jax.ShapeDtypeStruct((cols, width), wide),
            jax.ShapeDtypeStruct((tok_rows, pair), wide),
        ),
        in_specs=[pl.BlockSpec(memory_space=pl.ANY)] + [vmem] * 4,
        out_specs=(vmem, vmem),
        scratch_shapes=[
            pltpu.VMEM((2, rounds, half, tok_rows), low),
            pltpu.VMEM((2, rounds, 2 * zs, half, width), low),
            pltpu.VMEM((2, rounds, 2 * zs, half, width), low),
            pltpu.VMEM((2, rounds, zs, half, width), wide),
            pltpu.VMEM((2, rounds, zs, half, width), low),
            pltpu.VMEM((2, rounds, zs, half, width), low),
            pltpu.VMEM((2, rounds, zs - 1, half, width), low),
            pltpu.VMEM((2, rounds, zs - 1, half, width), low),
            pltpu.VMEM((n, BLOCK, pair), low),
            pltpu.VMEM((nb, BLOCK, pair), wide),
            pltpu.VMEM((tp - 1, nb, BLOCK, pair), wide),
            dma((2, rounds, 2 * zs)), dma((2, rounds, 2 * zs)),
            dma((2, rounds, zs)), dma((2, rounds, zs)),
            dma((2, rounds, zs - 1)), dma((2, rounds, zs - 1)),
            dma((n,)), dma((n,)),
            dma((tp - 1,)), dma((tp - 1,)),
            pltpu.VMEM((tok_rows, model_width), low), dma,
        ],
        compiler_params=pltpu.CompilerParams(
            collective_id=1, has_side_effects=True, vmem_limit_bytes=56 * 1024 * 1024
        ),
        name="reduce",
    )(normed, gq, own_part, back, asked)
    weight_grad, grad_keys, grad_values = pl.pallas_call(
        turn_kernel,
        out_shape=(
            jax.ShapeDtypeStruct((width, cols), wide),
            jax.ShapeDtypeStruct((BLOCK, tok_rows), wide),
            jax.ShapeDtypeStruct((BLOCK, tok_rows), wide),
        ),
        in_specs=[vmem] * 2,
        out_specs=(vmem, vmem, vmem),
        name="turn",
    )(turned, dkv)
    return (gq, grad_keys.T, grad_values.T, weight_grad)


def solution(mesh):
    placed = (
        P("kv", None),
        P("kv", "tp"),
        P("kv", None),
        P("kv", None),
        P("kv", "tp"),
        P("kv", "tp"),
        P("kv", "tp"),
        P("kv", None),
    )
    return jax.shard_map(
        functools.partial(shards, mesh.shape["kv"], mesh.shape["tp"]),
        mesh=mesh,
        in_specs=placed,
        out_specs=(P("kv", "tp"), P("kv", None), P("kv", None), P("kv", "tp")),
        check_vma=False,
    )
```
